256 devices in a mesh: ep: 16 (over y, x), tp: 16 (over z, core).
Axes of the slice: x: 4, y: 4, z: 8, core: 2. Of those that a mesh axis runs over, the one named last changes fastest.
Arguments:
- queries: bfloat16 [16384, 1024], P('ep', 'tp'), may hold values from -30 to 30
- key_vectors: bfloat16 [16384, 1024], P('ep', 'tp'), may hold values from -30 to 30
- value_vectors: bfloat16 [16384, 1024], P('ep', 'tp'), may hold values from -9 to 9
- cumulative_gate: float32 [16384, 16], P('ep', 'tp'), as said below
- out_weight: bfloat16 [1024, 2048], P('tp'), may hold values from -0.1875 to 0.1875
- expert_tokens: bfloat16 [24576, 2048], P(('ep', 'tp')), may hold values from -6 to 6
- norm_gain: float32 [2048], replicated, may hold values from 0.1 to 1.9
- gate_weight: bfloat16 [16, 2048, 2048], P('ep', None, 'tp'), may hold values from -0.375 to 0.375
- up_weight: bfloat16 [16, 2048, 2048], P('ep', None, 'tp'), may hold values from -0.375 to 0.375
- down_weight: bfloat16 [16, 2048, 2048], P('ep', 'tp'), may hold values from -0.015625 to 0.015625
- expert_choice: int32 [24576, 2], P(('ep', 'tp')), may hold values from 0 to 15, all different within a row; in each aligned block of 96 rows (0 to 95, 96 to 191, ...) at most 13 rows name the same one
- route_weights: float32 [24576, 2], P(('ep', 'tp')), may hold values from 0.2 to 1
Outputs:
- mixer_output: bfloat16 [16384, 2048], P(('ep', 'tp'))
- expert_output: bfloat16 [24576, 2048], P(('ep', 'tp'))
The draws below stay inside these ranges and needn't reach their ends.
Inputs may be any that keep to these rules, and one draw needn't show every extreme that they name: `cumulative_gate`: each head's values never rise from one position to the next. `expert_choice`: each row names 2 different experts; within the rows of one device no expert is named more than 13 times, and in some of them one expert exactly 13 times.
All inputs are finite; a program needn't handle non-finite values.
Results may differ from the reference program's by a relative error of at most 0.019.
Values may be sent and summed in bfloat16 or wider, within the bound.
A program may use at most 128 MiB of HBM per device.

```python
import math
import jax
import jax.numpy as jnp
import numpy as np
from jax import lax

D = 2048
HEAD_DIM = 64
HEAD_COUNT = 16
FF = 2048
EXPERTS = 16
TOPK = 2
TOK_DEV = 96
CAP = 13
ROWS = 1024
TOKEN_POSITIONS = 16384
EXP_TOKENS = 24576
N_TP = 16


def paired_vectors(key):
    full_width = HEAD_COUNT * HEAD_DIM
    query_key = jax.random.fold_in(key, 101)
    vector_key = jax.random.fold_in(key, 102)
    queries = jnp.clip(jax.random.normal(query_key, (TOKEN_POSITIONS, full_width), jnp.float32), -6.0, 6.0)
    vectors = jnp.clip(jax.random.normal(vector_key, (TOKEN_POSITIONS, full_width), jnp.float32), -6.0, 6.0)
    return (queries, vectors)


def draw_queries(key, part):
    return paired_vectors(key)[0].astype(jnp.bfloat16)


def draw_key_vectors(key, part):
    return paired_vectors(key)[1].astype(jnp.bfloat16)


def draw_cumulative_gate(key, part):
    fast_share = 0.5
    head_draw = jax.random.uniform(jax.random.fold_in(key, 201), (HEAD_COUNT,), jnp.float32)
    fast_rate = jnp.exp(jax.random.uniform(jax.random.fold_in(key, 202), (HEAD_COUNT,), jnp.float32, math.log(0.012), math.log(0.035)))
    slow_rate = jnp.exp(jax.random.uniform(jax.random.fold_in(key, 203), (HEAD_COUNT,), jnp.float32, math.log(0.1), math.log(0.5))) / TOKEN_POSITIONS
    head_rate = jnp.where(head_draw < fast_share, fast_rate, slow_rate)
    block_count = TOKEN_POSITIONS // ROWS
    block_factor = jnp.exp(jax.random.uniform(jax.random.fold_in(key, 204), (block_count,), jnp.float32, math.log(0.4), math.log(2.5)))
    position_factor = jnp.repeat(block_factor, ROWS)
    roughness = jax.random.uniform(jax.random.fold_in(key, 205), (TOKEN_POSITIONS, HEAD_COUNT), jnp.float32, 0.3, 1.7)
    logarithm_gate = -head_rate[None, :] * position_factor[:, None] * roughness
    spike_rows = jax.random.randint(jax.random.fold_in(key, 206), (3,), 0, TOKEN_POSITIONS)
    spike_loss = jax.random.uniform(jax.random.fold_in(key, 207), (3, HEAD_COUNT), jnp.float32, 0.2, 0.4)
    logarithm_gate = logarithm_gate.at[spike_rows].add(jnp.log1p(-spike_loss))
    return jnp.cumsum(logarithm_gate, axis=0)


def block_levels(key, dims, cuts, smallest, high):
    loudness = 1.0
    for position, shards_of in cuts:
        draws = jax.random.uniform(jax.random.fold_in(jax.random.fold_in(key, 6), position), (shards_of,), jnp.float32, smallest / len(cuts), high / len(cuts))
        loudness = loudness * jnp.repeat(jnp.exp(draws), dims[position] // shards_of).reshape((-1,) + (1,) * (len(dims) - 1 - position))
    return loudness


def deal_out(stream_key, own, number, rows, amount, top, limit, lean):
    order = jax.random.permutation(stream_key, amount)
    crowded, usual = shares(amount, rows * top, limit, lean, True), shares(amount, rows * top, limit, lean, False)
    places = jnp.arange(amount)

    def named(tallies, rotation):
        used = int((tallies > 0).sum())
        fixed = max(1, used // 4)
        moved = fixed + (places - fixed + rotation * (used - fixed)) % max(1, amount - fixed)
        return jnp.zeros((amount,), jnp.int32).at[order[jnp.where(places < fixed, places, moved)]].set(jnp.asarray(tallies, jnp.int32))

    tallies = jnp.where(number % 4 == 0, named(crowded, number // 4), named(usual, number - number // 4 - 1))
    mixed = jax.random.permutation(jax.random.fold_in(own, 3), amount)
    giver, sink = mixed[0:amount // 2 * 2:2], mixed[1:amount // 2 * 2:2]
    room = jnp.minimum(tallies[giver] - 1, limit - tallies[sink]) // 2
    room = jnp.where((giver == order[0]) | (sink == order[0]) | (tallies[sink] == 0), 0, jnp.maximum(room, 0))
    moved = jax.random.randint(jax.random.fold_in(own, 4), (amount // 2,), 0, 1 << 20) % (room + 1)
    tallies = tallies.at[giver].add(-moved).at[sink].add(moved)
    items = jnp.searchsorted(jnp.cumsum(tallies), jnp.arange(rows * top), side="right").astype(jnp.int32)
    table = items.reshape(top, rows).T
    table = table[jax.random.permutation(jax.random.fold_in(own, 1), rows)]
    rotation = jax.random.randint(jax.random.fold_in(own, 2), (rows, 1), 0, top)
    return jnp.take_along_axis(table, (jnp.arange(top)[None, :] + rotation) % top, axis=1)


def shares(amount, total, bound, skew, full):
    weights = [(1 << 20) // math.isqrt(grade ** skew) + 1 for grade in range(1, amount + 1)]
    largest = bound if full else min(bound, max(-(-total // amount), total * weights[0] // sum(weights)))
    least = 1 if total - largest >= amount - 1 else 0
    counts, surplus = [largest] + [least] * (amount - 1), total - largest - least * (amount - 1)
    while surplus > 0:
        free = [i for i in range(1, amount) if counts[i] < largest] or [i for i in range(1, amount) if counts[i] < bound]
        mass, remaining = sum([weights[i] for i in free]), surplus
        for i in free:
            more = min(bound - counts[i], max(1, remaining * weights[i] // mass), surplus)
            counts[i] = counts[i] + more
            surplus = surplus - more
    return np.array(counts)


def scatter_about(own_key, dims, scale, bound, shards=(), held_as=jnp.bfloat16):
    array = jax.random.normal(own_key, dims, jnp.float32) * scale
    if len(shards) > 0:
        array = block_levels(own_key, dims, shards, -0.22, 0.18) * array
    return jnp.clip(array, min=-bound, max=bound).astype(held_as)


def setup_inputs(seed: int = 0) -> dict:
    keys = jax.random.split(jax.random.key(seed), 13)
    queries = draw_queries(jax.random.fold_in(keys[12], 71), 0)
    key_vectors = draw_key_vectors(jax.random.fold_in(keys[12], 71), 0)
    value_vectors = scatter_about(keys[2], (TOKEN_POSITIONS, HEAD_COUNT * HEAD_DIM), 1.5, 9.0, ((0, 16), (1, 16)))
    cumulative_gate = draw_cumulative_gate(jax.random.fold_in(keys[12], 71), 0)
    out_weight = scatter_about(keys[4], (HEAD_COUNT * HEAD_DIM, D), (HEAD_COUNT * HEAD_DIM) ** -0.5, 0.1875, ((0, 16),))
    expert_tokens = scatter_about(keys[5], (EXP_TOKENS, D), 1.0, 6.0, ((0, 256),))
    norm_gain = jnp.clip(1.0 + 0.18 * jax.random.normal(keys[6], (D,), jnp.float32), 0.1, 1.9)
    gate_weight = scatter_about(keys[7], (EXPERTS, D, FF), (D // 9) ** -0.5, 0.375, ((0, 16), (2, 16)))
    up_weight = scatter_about(keys[8], (EXPERTS, D, FF), (D // 9) ** -0.5, 0.375, ((0, 16), (2, 16)))
    down_weight = scatter_about(keys[9], (EXPERTS, FF, D), (FF * 64) ** -0.5, 0.015625, ((0, 16), (1, 16)))
    expert_choice_keys = jax.random.split(jax.random.fold_in(keys[10], 1), EXP_TOKENS // TOK_DEV)
    expert_choice_turns = jax.random.permutation(jax.random.fold_in(keys[10], 3), EXP_TOKENS // TOK_DEV)
    expert_choice = jax.vmap(lambda own, number: deal_out(jax.random.fold_in(keys[10], 2), own, number, TOK_DEV, EXPERTS, TOPK, CAP, 1))(expert_choice_keys, expert_choice_turns).reshape((EXP_TOKENS, TOPK))
    route_weights = jnp.clip(0.2 + 0.8 * jax.random.uniform(keys[11], (EXP_TOKENS, TOPK), jnp.float32) ** block_levels(keys[11], (EXP_TOKENS, TOPK), ((0, 256),), -0.2, 0.2), 0.2, 1.0)
    return {"queries": queries, "key_vectors": key_vectors, "value_vectors": value_vectors, "cumulative_gate": cumulative_gate, "out_weight": out_weight, "expert_tokens": expert_tokens, "norm_gain": norm_gain, "gate_weight": gate_weight, "up_weight": up_weight, "down_weight": down_weight, "expert_choice": expert_choice, "route_weights": route_weights}


eps_norm = 1e-05
clamp_limit = 7.0
sig_alpha = 1.702

def mixer_part(queries, key_vectors, value_vectors, cumulative_gate, out_weight):
    total_rows = queries.shape[0]
    block_size = min(512, total_rows)
    block_count = total_rows // block_size
    score_scale = 1.0 / math.sqrt(HEAD_DIM)
    key_pos = jnp.arange(total_rows, dtype=jnp.int32)

    def single_head(head_index):
        first_column = (head_index * HEAD_DIM).astype(jnp.int32)
        head_queries = lax.dynamic_slice_in_dim(queries, first_column, HEAD_DIM, 1)
        head_keys = lax.dynamic_slice_in_dim(key_vectors, first_column, HEAD_DIM, 1)
        head_values = lax.dynamic_slice_in_dim(value_vectors, first_column, HEAD_DIM, 1)
        head_gates = lax.dynamic_slice_in_dim(cumulative_gate, head_index.astype(jnp.int32), 1, 1)[:, 0]

        def one_block(block_index):
            row_start = (block_index * block_size).astype(jnp.int32)
            block_queries = lax.dynamic_slice_in_dim(head_queries, row_start, block_size, 0)
            block_gates = lax.dynamic_slice_in_dim(head_gates, row_start, block_size, 0)
            scores = jnp.dot(block_queries, head_keys.T, preferred_element_type=jnp.float32) * score_scale
            scores = scores + block_gates[:, None] - head_gates[None, :]
            query_pos = row_start + jnp.arange(block_size, dtype=jnp.int32)
            causal = key_pos[None, :] <= query_pos[:, None]
            scores = jnp.where(causal, scores, -jnp.inf)
            row_peak = lax.optimization_barrier(jnp.max(scores, axis=1, keepdims=True))
            weights = jnp.where(causal, jnp.exp(scores - row_peak), 0.0)
            numer = jnp.dot(weights.astype(jnp.bfloat16), head_values, preferred_element_type=jnp.float32)
            return (numer / lax.optimization_barrier(jnp.sum(weights, axis=1, keepdims=True))).astype(jnp.bfloat16)
        return lax.map(one_block, jnp.arange(block_count, dtype=jnp.int32)).reshape(total_rows, HEAD_DIM)
    per_head = lax.map(single_head, jnp.arange(HEAD_COUNT, dtype=jnp.int32))
    attention = jnp.transpose(per_head, (1, 0, 2)).reshape(total_rows, HEAD_COUNT * HEAD_DIM)
    group_width = HEAD_COUNT // N_TP * HEAD_DIM

    def add_group(running_total, group_index):
        first_column = (group_index * group_width).astype(jnp.int32)
        columns = lax.dynamic_slice_in_dim(attention, first_column, group_width, 1)
        weight_rows = lax.dynamic_slice_in_dim(out_weight, first_column, group_width, 0)
        partial_sum = jnp.dot(columns, weight_rows, preferred_element_type=jnp.float32).astype(jnp.bfloat16)
        partial_sum = lax.optimization_barrier(partial_sum)
        return (running_total + partial_sum.astype(jnp.float32), None)
    summed, unused = lax.scan(add_group, jnp.zeros((total_rows, D), jnp.float32), jnp.arange(N_TP, dtype=jnp.int32))
    return summed.astype(jnp.bfloat16)

def expert_part(expert_tokens, norm_gain, gate_weight, up_weight, down_weight, expert_choice, route_weights):
    total_rows = expert_tokens.shape[0]
    block_count = total_rows // TOK_DEV
    tokens_float = expert_tokens.astype(jnp.float32)
    normed = (tokens_float * lax.rsqrt(lax.optimization_barrier(jnp.mean(tokens_float * tokens_float, axis=1, keepdims=True)) + eps_norm) * norm_gain).astype(jnp.bfloat16)
    flat_ids = expert_choice.reshape(block_count, TOK_DEV * TOPK).astype(jnp.int32)
    one_hot = (flat_ids[:, :, None] == jnp.arange(EXPERTS, dtype=jnp.int32)[None, None, :]).astype(jnp.int32)
    slot_rank = lax.optimization_barrier(jnp.sum((jnp.cumsum(one_hot, axis=1) - one_hot) * one_hot, axis=2))
    block_ids = jnp.arange(block_count, dtype=jnp.int32)[:, None]
    destination = (flat_ids * (block_count * CAP) + block_ids * CAP + slot_rank).reshape(-1)
    token_ids = (block_ids * TOK_DEV + jnp.arange(TOK_DEV * TOPK, dtype=jnp.int32)[None, :] // TOPK).reshape(-1)
    slot_rows = jnp.zeros((EXPERTS * block_count * CAP, D), jnp.bfloat16).at[destination].set(normed[token_ids])
    slot_rows = slot_rows.reshape(EXPERTS, block_count * CAP, D)
    unit_group = FF // N_TP

    def single_expert(operands):
        rows_in, gate_matrix, up_matrix, down_matrix = operands
        gate_pre = jnp.minimum(jnp.dot(rows_in, gate_matrix, preferred_element_type=jnp.float32), clamp_limit)
        up_pre = jnp.clip(jnp.dot(rows_in, up_matrix, preferred_element_type=jnp.float32), -clamp_limit, clamp_limit)
        activation = (gate_pre * jax.nn.sigmoid(sig_alpha * gate_pre) * (up_pre + 1.0)).astype(jnp.bfloat16)

        def add_group(running_total, group_index):
            first_unit = (group_index * unit_group).astype(jnp.int32)
            columns = lax.dynamic_slice_in_dim(activation, first_unit, unit_group, 1)
            weight_rows = lax.dynamic_slice_in_dim(down_matrix, first_unit, unit_group, 0)
            partial_sum = jnp.dot(columns, weight_rows, preferred_element_type=jnp.float32).astype(jnp.bfloat16)
            partial_sum = lax.optimization_barrier(partial_sum)
            return (running_total + partial_sum.astype(jnp.float32), None)
        summed, unused = lax.scan(add_group, jnp.zeros((rows_in.shape[0], D), jnp.float32), jnp.arange(N_TP, dtype=jnp.int32))
        return summed.astype(jnp.bfloat16)
    results = lax.map(single_expert, (slot_rows, gate_weight, up_weight, down_weight)).reshape(EXPERTS * block_count * CAP, D)
    picked = results[destination].astype(jnp.float32).reshape(total_rows, TOPK, D)
    return lax.optimization_barrier(jnp.sum(picked * route_weights[:, :, None], axis=1)).astype(jnp.bfloat16)

def reference(queries, key_vectors, value_vectors, cumulative_gate, out_weight, expert_tokens, norm_gain, gate_weight, up_weight, down_weight, expert_choice, route_weights):
    mixer_output = mixer_part(queries, key_vectors, value_vectors, cumulative_gate, out_weight)
    expert_output = expert_part(expert_tokens, norm_gain, gate_weight, up_weight, down_weight, expert_choice, route_weights)
    return (mixer_output, expert_output)
```

```python
import functools
import math

import jax
import jax.numpy as jnp
from jax import lax
from jax.experimental import pallas as pl
from jax.experimental.pallas import tpu as pltpu
from jax.sharding import PartitionSpec as P

EXPERTS = 16
CAP = 13
SLOT = 16
TQ = 256

eps_norm = 1e-05
clamp_limit = 7.0
sig_alpha = 1.702
floor_score = -1e30


def attend_block(q_ref, cq_ref, kv, ck_row, m_ref, l_ref, acc_ref, diagonal):
    width = kv.shape[0]

    def one_tile(i, carry):
        rows = pl.ds(pl.multiple_of(i * TQ, TQ), TQ)
        s = lax.dot_general(
            q_ref[rows, :], kv, (((1,), (1,)), ((), ())), preferred_element_type=jnp.float32
        )
        s = s + (cq_ref[rows, :] - ck_row)
        if diagonal:
            q_pos = i * TQ + lax.broadcasted_iota(jnp.int32, (TQ, width), 0)
            k_pos = lax.broadcasted_iota(jnp.int32, (TQ, width), 1)
            s = jnp.where(k_pos <= q_pos, s, floor_score)
        top = jnp.max(s, axis=1, keepdims=True)
        if diagonal:
            p = jnp.exp(s - top)
            m_ref[rows, :] = jnp.broadcast_to(top, (TQ, 128))
            l_ref[rows, :] = jnp.broadcast_to(jnp.sum(p, axis=1, keepdims=True), (TQ, 128))
            acc_ref[rows, :] = jnp.dot(
                p.astype(jnp.bfloat16), kv, preferred_element_type=jnp.float32
            )
        else:
            old = m_ref[rows, :]
            new = jnp.maximum(old, top)
            shrink = jnp.exp(old - new)
            p = jnp.exp(s - new[:, :1])
            m_ref[rows, :] = new
            l_ref[rows, :] = l_ref[rows, :] * shrink + jnp.sum(p, axis=1, keepdims=True)
            acc_ref[rows, :] = acc_ref[rows, :] * shrink + jnp.dot(
                p.astype(jnp.bfloat16), kv, preferred_element_type=jnp.float32
            )
        return carry

    lax.fori_loop(0, q_ref.shape[0] // TQ, one_tile, 0)


def gate_row(tile):
    return jnp.concatenate([tile[r : r + 1, :] for r in range(tile.shape[0])], axis=1)


def attention_kernel(q_ref, cq_ref, kv_ref, ck_ref, out_ref, m_ref, l_ref, acc_ref):
    me = lax.axis_index("ep")
    attend_block(q_ref, cq_ref, kv_ref[me], gate_row(ck_ref[me]), m_ref, l_ref, acc_ref, True)

    def step(k, carry):
        j = me - k
        attend_block(q_ref, cq_ref, kv_ref[j], gate_row(ck_ref[j]), m_ref, l_ref, acc_ref, False)
        return carry

    lax.fori_loop(1, me + 1, step, 0)
    out_ref[...] = (acc_ref[...] / l_ref[...])[:, 64:].astype(jnp.bfloat16)


def activate(g, u):
    g = jnp.minimum(g, clamp_limit)
    u = jnp.clip(u, -clamp_limit, clamp_limit)
    return (g * jax.nn.sigmoid(sig_alpha * g) * (u + 1.0)).astype(jnp.bfloat16)


def expert_kernel(x_ref, g_ref, u_ref, d_ref, out_ref, acc_ref):
    step = pl.program_id(0)
    x = x_ref[...]
    g = jnp.dot(x, g_ref[...], preferred_element_type=jnp.float32)
    u = jnp.dot(x, u_ref[...], preferred_element_type=jnp.float32)
    part = jnp.dot(activate(g, u), d_ref[...], preferred_element_type=jnp.float32)

    @pl.when(step == 0)
    def _():
        acc_ref[...] = part

    @pl.when(step > 0)
    def _():
        acc_ref[...] += part

    @pl.when(step == pl.num_programs(0) - 1)
    def _():
        out_ref[...] = acc_ref[...].astype(jnp.bfloat16)


def route(expert_choice, route_weights):
    flat_ids = expert_choice.reshape(-1)
    one_hot = (flat_ids[:, None] == jnp.arange(EXPERTS, dtype=jnp.int32)[None, :]).astype(jnp.int32)
    slot_rank = jnp.sum((jnp.cumsum(one_hot, axis=0) - one_hot) * one_hot, axis=1)
    slot_ids = (flat_ids * SLOT + slot_rank).reshape(expert_choice.shape)
    table = slot_ids[:, :, None] == jnp.arange(EXPERTS * SLOT, dtype=jnp.int32)[None, None, :]
    placing = jnp.sum(table.astype(jnp.bfloat16), axis=1)
    combine = jnp.sum(jnp.where(table, route_weights[:, :, None], 0.0), axis=1)
    return placing, combine


def local(
    queries,
    key_vectors,
    value_vectors,
    cumulative_gate,
    out_weight,
    expert_tokens,
    norm_gain,
    gate_weight,
    up_weight,
    down_weight,
    expert_choice,
    route_weights,
):
    width = expert_tokens.shape[1]
    block_rows = queries.shape[0]
    n_ep = lax.axis_size("ep")
    n_tp = lax.axis_size("tp")
    kv = jnp.concatenate([key_vectors, value_vectors], axis=1)
    kv_all = lax.all_gather(kv, "ep", axis=0, tiled=True).reshape(n_ep, block_rows, 128)
    gate_tile = cumulative_gate.reshape(block_rows // 128, 128)
    gates_all = lax.all_gather(gate_tile, "ep", axis=0)
    gate_all = lax.all_gather(gate_weight[0], "tp", axis=0, tiled=True)
    up_all = lax.all_gather(up_weight[0], "tp", axis=0, tiled=True)
    down_all = lax.all_gather(down_weight[0], "tp", axis=0, tiled=True)
    out_all = lax.all_gather(out_weight, "tp", axis=0, tiled=True)

    tokens_float = expert_tokens.astype(jnp.float32)
    normed = (
        tokens_float
        * lax.rsqrt(jnp.mean(tokens_float * tokens_float, axis=1, keepdims=True) + eps_norm)
        * norm_gain
    ).astype(jnp.bfloat16)
    placing, combine = route(expert_choice, route_weights)
    outgoing = jnp.einsum("ts,td->sd", placing, normed, preferred_element_type=jnp.float32).astype(
        jnp.bfloat16
    )
    arrived = lax.all_to_all(
        outgoing.reshape(EXPERTS, SLOT, width), "ep", split_axis=0, concat_axis=0, tiled=True
    ).reshape(-1, width)

    head = queries.shape[1]
    q_wide = jnp.pad(queries * jnp.bfloat16(1.0 / math.sqrt(head)), ((0, 0), (0, 128 - head)))
    attention = pl.pallas_call(
        attention_kernel,
        out_shape=jax.ShapeDtypeStruct((block_rows, head), jnp.bfloat16),
        in_specs=[pl.BlockSpec(memory_space=pltpu.VMEM)] * 4,
        out_specs=pl.BlockSpec(memory_space=pltpu.VMEM),
        scratch_shapes=[pltpu.VMEM((block_rows, 128), jnp.float32)] * 3,
        compiler_params=pltpu.CompilerParams(vmem_limit_bytes=40 * 2**20),
        cost_estimate=pl.CostEstimate(flops=10**10, bytes_accessed=6 * 10**6, transcendentals=0),
        name="attend",
    )(q_wide, cumulative_gate, kv_all, gates_all)
    pieces = lax.all_to_all(
        attention.reshape(n_tp, block_rows // n_tp, head), "tp", split_axis=0, concat_axis=0
    )
    heads = pieces.transpose(1, 0, 2).reshape(block_rows // n_tp, n_tp * head)
    mixer_output = jnp.dot(heads, out_all, preferred_element_type=jnp.float32).astype(jnp.bfloat16)

    units = gate_weight.shape[2]
    rows = arrived.shape[0]
    results = pl.pallas_call(
        expert_kernel,
        grid=(n_tp,),
        out_shape=jax.ShapeDtypeStruct((rows, width), jnp.bfloat16),
        in_specs=[
            pl.BlockSpec((rows, width), lambda i: (0, 0)),
            pl.BlockSpec((width, units), lambda i: (i, 0)),
            pl.BlockSpec((width, units), lambda i: (i, 0)),
            pl.BlockSpec((units, width), lambda i: (i, 0)),
        ],
        out_specs=pl.BlockSpec((rows, width), lambda i: (0, 0)),
        scratch_shapes=[pltpu.VMEM((rows, width), jnp.float32)],
        compiler_params=pltpu.CompilerParams(vmem_limit_bytes=40 * 2**20),
        cost_estimate=pl.CostEstimate(flops=10**10, bytes_accessed=26 * 10**6, transcendentals=0),
        name="experts",
    )(arrived, gate_all, up_all, down_all)
    returned = lax.all_to_all(
        results.reshape(n_ep, SLOT, width), "ep", split_axis=0, concat_axis=0, tiled=True
    ).reshape(-1, width)
    expert_output = jnp.dot(
        combine, returned.astype(jnp.float32), precision=lax.Precision.HIGHEST
    ).astype(jnp.bfloat16)
    return (mixer_output, expert_output)


def solution(mesh):
    placed = (
        P("ep", "tp"),
        P("ep", "tp"),
        P("ep", "tp"),
        P("ep", "tp"),
        P("tp", None),
        P(("ep", "tp"), None),
        P(),
        P("ep", None, "tp"),
        P("ep", None, "tp"),
        P("ep", "tp", None),
        P(("ep", "tp"), None),
        P(("ep", "tp"), None),
    )
    return jax.shard_map(
        local,
        mesh=mesh,
        in_specs=placed,
        out_specs=(P(("ep", "tp"), None), P(("ep", "tp"), None)),
        check_vma=False,
    )
```

```python
import functools
import math

import jax
import jax.numpy as jnp
from jax import lax
from jax.experimental import pallas as pl
from jax.experimental.pallas import tpu as pltpu
from jax.sharding import PartitionSpec as P

SLOT = 16
TQ = 256
HEAD = 64
MESH = pl.DeviceIdType.MESH

eps_norm = 1e-05
clamp_limit = 7.0
sig_alpha = 1.702
floor_score = -1e30


def gate_row(tile):
    return jnp.concatenate([tile[r : r + 1, :] for r in range(tile.shape[0])], axis=1)


def activate(g, u):
    g = jnp.minimum(g, clamp_limit)
    u = jnp.clip(u, -clamp_limit, clamp_limit)
    return (g * jax.nn.sigmoid(sig_alpha * g) * (u + 1.0)).astype(jnp.bfloat16)


def attend_block(q_ref, cq_ref, kv_ref, ck_ref, m_ref, l_ref, acc_ref, diagonal):
    width = kv_ref.shape[0]
    tile = min(TQ, q_ref.shape[0])
    ck_row = gate_row(ck_ref[...])

    def one_tile(i, carry):
        rows = pl.ds(pl.multiple_of(i * tile, tile), tile)
        kv = kv_ref[...]
        s = lax.dot_general(
            q_ref[rows, :], kv, (((1,), (1,)), ((), ())), preferred_element_type=jnp.float32
        )
        s = s + (cq_ref[rows, :] - ck_row)
        if diagonal:
            q_pos = i * tile + lax.broadcasted_iota(jnp.int32, (tile, width), 0)
            k_pos = lax.broadcasted_iota(jnp.int32, (tile, width), 1)
            s = jnp.where(k_pos <= q_pos, s, floor_score)
        top = jnp.max(s, axis=1, keepdims=True)
        if diagonal:
            p = jnp.exp(s - top)
            m_ref[rows, :] = jnp.broadcast_to(top, (tile, 128))
            l_ref[rows, :] = jnp.broadcast_to(jnp.sum(p, axis=1, keepdims=True), (tile, 128))
            acc_ref[rows, :] = jnp.dot(
                p.astype(jnp.bfloat16), kv, preferred_element_type=jnp.float32
            )
        else:
            old = m_ref[rows, :]
            new = jnp.maximum(old, top)
            shrink = jnp.exp(old - new)
            p = jnp.exp(s - new[:, :1])
            m_ref[rows, :] = new
            l_ref[rows, :] = l_ref[rows, :] * shrink + jnp.sum(p, axis=1, keepdims=True)
            acc_ref[rows, :] = acc_ref[rows, :] * shrink + jnp.dot(
                p.astype(jnp.bfloat16), kv, preferred_element_type=jnp.float32
            )
        return carry

    lax.fori_loop(0, q_ref.shape[0] // tile, one_tile, 0)


def body(
    n_ep,
    n_tp,
    q_ref,
    cq_ref,
    kv_ref,
    ck_ref,
    wg_ref,
    wu_ref,
    wd_ref,
    ow_ref,
    og_ref,
    comb_ref,
    mix_ref,
    eo_ref,
    kv_all,
    ck_all,
    rg,
    ru,
    rd,
    lg,
    lu,
    ld,
    x,
    acc,
    p_send,
    p_recv,
    res,
    ret,
    osl,
    w_all,
    att_send,
    att_in,
    mix_acc,
    mp_send,
    mp_recv,
    m_ref,
    l_ref,
    att_acc,
    s_kv,
    r_kv,
    s_ck,
    r_ck,
    s_og,
    r_og,
    s_res,
    r_res,
    s_osl,
    r_osl,
    s_w,
    r_w,
    s_att,
    r_att,
    s_ring,
    r_ring,
    s_pt,
    r_pt,
):
    nz = n_tp // 2
    hops = nz // 2 - 1
    ep = lax.axis_index("ep")
    tp = lax.axis_index("tp")
    z = lax.div(tp, 2)
    core = lax.rem(tp, 2)
    right = lax.rem(tp + 2, n_tp)
    left = lax.rem(tp + n_tp - 2, n_tp)
    partner = tp + 1 - 2 * core
    width = wg_ref.shape[0]
    col = width // n_ep
    t_dev = mp_send.shape[0]
    half_units = ld.shape[0] // 2

    def ep_peer(d):
        return lax.rem(ep + d, n_ep)

    def z_peer(d):
        return lax.rem(z + d, nz)

    def ep_copy(src, dst, send, recv, peer):
        return pltpu.make_async_remote_copy(
            src_ref=src, dst_ref=dst, send_sem=send, recv_sem=recv,
            device_id={"ep": peer}, device_id_type=MESH,
        )

    def tp_copy(src, dst, send, recv, peer):
        return pltpu.make_async_remote_copy(
            src_ref=src, dst_ref=dst, send_sem=send, recv_sem=recv,
            device_id={"tp": peer}, device_id_type=MESH,
        )

    def kv_copy(slot, peer):
        return ep_copy(kv_ref, kv_all.at[slot], s_kv.at[peer], r_kv.at[slot], peer)

    def ck_copy(slot, peer):
        return ep_copy(ck_ref, ck_all.at[slot], s_ck.at[peer], r_ck.at[slot], peer)

    def og_copy(slot, peer):
        return ep_copy(og_ref.at[peer], x.at[0, slot], s_og.at[peer], r_og.at[slot], peer)

    def res_copy(slot, peer):
        return ep_copy(res.at[peer], ret.at[slot], s_res.at[peer], r_res.at[slot], peer)

    def w_copy(slot, peer):
        return ep_copy(osl, w_all.at[slot], s_w.at[peer], r_w.at[slot], peer)

    my_cols = pl.ds(pl.multiple_of(ep * col, col), col)

    def osl_copy(slot, pz):
        return tp_copy(
            ow_ref.at[:, my_cols], osl.at[slot], s_osl.at[pz], r_osl.at[slot], 2 * pz + core
        )

    def att_copy(slot, pz):
        return tp_copy(
            att_send.at[pz], att_in.at[slot], s_att.at[pz], r_att.at[slot], 2 * pz + core
        )

    def pt_copy(src, dst, n):
        return tp_copy(src, dst, s_pt.at[n], r_pt.at[n], partner)

    own = (wg_ref, wu_ref, wd_ref)
    slots = (rg, ru, rd)
    peers = (right, left)

    def first_copy(direction, a):
        return tp_copy(
            own[a], slots[a].at[direction, 0], s_ring.at[direction, 0, a],
            r_ring.at[direction, 0, a], peers[direction],
        )

    def ring_copy(direction, h, a):
        return tp_copy(
            slots[a].at[direction, h - 1], slots[a].at[direction, h],
            s_ring.at[direction, h, a], r_ring.at[direction, h, a], peers[direction],
        )

    def last_copy(direction, a):
        src = slots[a].at[direction, hops - 1]
        if a == 0:
            dst = lg
        elif a == 1:
            dst = lu
        else:
            part = pl.ds(direction * half_units, half_units)
            src, dst = src.at[part], ld.at[part]
        return tp_copy(
            src, dst, s_ring.at[direction, hops, a], r_ring.at[direction, hops, a],
            peers[direction],
        )

    last_parts = ((0, 0), (1, 1), (0, 2), (1, 2))

    barrier = pltpu.get_barrier_semaphore()

    def greet_ep(d, carry):
        pl.semaphore_signal(barrier, inc=1, device_id={"ep": ep_peer(d)}, device_id_type=MESH)
        return carry

    def greet_z(d, carry):
        pl.semaphore_signal(
            barrier, inc=1, device_id={"tp": 2 * z_peer(d) + core}, device_id_type=MESH
        )
        return carry

    lax.fori_loop(1, n_ep, greet_ep, 0)
    lax.fori_loop(1, nz, greet_z, 0)
    pl.semaphore_signal(barrier, inc=1, device_id={"tp": partner}, device_id_type=MESH)
    pl.semaphore_wait(barrier, n_ep - 1 + nz - 1 + 1)

    def each(start, stop, fn):
        def run(d, carry):
            fn(d)
            return carry

        lax.fori_loop(start, stop, run, 0)

    each(1, nz, lambda d: osl_copy(z, z_peer(d)).start())
    for a in range(3):
        for direction in range(2):
            first_copy(direction, a).start()
    each(1, n_ep, lambda d: og_copy(ep, ep_peer(d)).start())

    def send_kv(d):
        kv_copy(ep, ep + d).start()
        ck_copy(ep, ep + d).start()

    each(1, n_ep - ep, send_kv)

    x[0, ep] = og_ref[ep]
    osl[z] = ow_ref[:, my_cols]

    attend_block(q_ref, cq_ref, kv_ref, ck_ref, m_ref, l_ref, att_acc, True)

    def attend_step(k):
        @pl.when(k <= ep)
        def _():
            j = ep - k
            kv_copy(j, j).wait_recv()
            ck_copy(j, j).wait_recv()
            attend_block(
                q_ref, cq_ref, kv_all.at[j], ck_all.at[j], m_ref, l_ref, att_acc, False
            )

    def expert_step(g_ref, u_ref, d_ref, first):
        for half in range(2):
            rows = x[half].reshape(n_ep * SLOT, width)
            g = jnp.dot(rows, g_ref[...], preferred_element_type=jnp.float32)
            u = jnp.dot(rows, u_ref[...], preferred_element_type=jnp.float32)
            part = jnp.dot(activate(g, u), d_ref[...], preferred_element_type=jnp.float32)
            if first:
                acc[half] = part
            else:
                acc[half] += part

    per_step = -(-n_ep // (3 * hops))

    def hop_step(h, carry):
        for a in range(3):
            for direction in range(2):
                @pl.when(h == 0)
                def _():
                    first_copy(direction, a).wait_recv()

                @pl.when(h > 0)
                def _():
                    ring_copy(direction, h, a).wait_recv()

                @pl.when(h < hops - 1)
                def _():
                    ring_copy(direction, h + 1, a).start()

                if (direction, a) in last_parts:
                    @pl.when(h == hops - 1)
                    def _():
                        last_copy(direction, a).start()

            if a == 1:
                @pl.when(h == 0)
                def _():
                    each(1, n_ep, lambda d: og_copy(ep_peer(d), ep_peer(d)).wait_recv())
                    pt_copy(x.at[0], x.at[1], 0).start()

            if a == 2:
                @pl.when(h == 0)
                def _():
                    each(1, nz, lambda d: osl_copy(z_peer(d), z_peer(d)).wait_recv())
                    each(1, n_ep, lambda d: w_copy(ep, ep_peer(d)).start())
                    w_all[ep] = osl[...]

            for i in range(per_step):
                attend_step((h * 3 + a) * per_step + i + 1)

        @pl.when(h == 0)
        def _():
            pt_copy(x.at[0], x.at[1], 0).wait_recv()
            expert_step(wg_ref, wu_ref, wd_ref, True)

        for direction in range(2):
            expert_step(
                rg.at[direction, h], ru.at[direction, h], rd.at[direction, h], False
            )
        return carry

    lax.fori_loop(0, hops, hop_step, 0)

    for pz in range(nz):
        rows = pl.ds(pz * 2 * t_dev, 2 * t_dev)
        o = (att_acc[rows, :] / l_ref[rows, :])[:, HEAD:]
        att_send[pz] = jnp.concatenate([o[:t_dev], o[t_dev:]], axis=1).astype(jnp.bfloat16)
    each(1, nz, lambda d: att_copy(z, z_peer(d)).start())
    att_in[z] = att_send[z]
    each(1, nz, lambda d: att_copy(z_peer(d), z_peer(d)).wait_recv())
    each(1, n_ep, lambda d: w_copy(ep_peer(d), ep_peer(d)).wait_recv())
    got = [att_in[pz].astype(jnp.float32) for pz in range(nz)]
    heads = jnp.concatenate(
        [
            jnp.concatenate([t[:, :HEAD] for t in got], axis=1),
            jnp.concatenate([t[:, HEAD:] for t in got], axis=1),
        ],
        axis=0,
    ).astype(jnp.bfloat16)

    def project(e, carry):
        piece = w_all[e].reshape(nz * HEAD, col)
        mix_acc[:, pl.ds(pl.multiple_of(e * col, col), col)] = jnp.dot(
            heads, piece, preferred_element_type=jnp.float32
        )
        return carry

    lax.fori_loop(0, n_ep, project, 0)
    theirs = pl.ds(pl.multiple_of((1 - core) * t_dev, t_dev), t_dev)
    mine = pl.ds(pl.multiple_of(core * t_dev, t_dev), t_dev)
    mp_send[...] = mix_acc[theirs, :].astype(jnp.bfloat16)
    pt_copy(mp_send, mp_recv, 1).start()

    last_copy(0, 0).wait_recv()
    last_copy(1, 1).wait_recv()
    acts = []
    for half in (1, 0):
        rows = x[half].reshape(n_ep * SLOT, width)
        g = jnp.dot(rows, lg[...], preferred_element_type=jnp.float32)
        u = jnp.dot(rows, lu[...], preferred_element_type=jnp.float32)
        acts.append(activate(g, u))
    pt_copy(mp_send, mp_recv, 1).wait_recv()
    mix_ref[...] = (mix_acc[mine, :] + mp_recv[...].astype(jnp.float32)).astype(jnp.bfloat16)
    last_copy(0, 2).wait_recv()
    last_copy(1, 2).wait_recv()
    p_send[...] = (
        acc[1] + jnp.dot(acts[0], ld[...], preferred_element_type=jnp.float32)
    ).astype(jnp.bfloat16)
    pt_copy(p_send, p_recv, 2).start()
    acc[0] += jnp.dot(acts[1], ld[...], preferred_element_type=jnp.float32)
    pt_copy(p_send, p_recv, 2).wait_recv()
    res[...] = (
        (acc[0] + p_recv[...].astype(jnp.float32))
        .astype(jnp.bfloat16)
        .reshape(n_ep, SLOT, width)
    )
    each(1, n_ep, lambda d: res_copy(ep, ep_peer(d)).start())
    ret[ep] = res[ep]

    each(1, nz, lambda d: osl_copy(z, z_peer(d)).wait_send())
    each(1, nz, lambda d: att_copy(z, z_peer(d)).wait_send())
    for a in range(3):
        for direction in range(2):
            first_copy(direction, a).wait_send()
            each(1, hops, lambda h: ring_copy(direction, h, a).wait_send())
    for direction, a in last_parts:
        last_copy(direction, a).wait_send()
    each(1, n_ep, lambda d: og_copy(ep, ep_peer(d)).wait_send())
    each(1, n_ep, lambda d: w_copy(ep, ep_peer(d)).wait_send())

    def sent_kv(d):
        kv_copy(ep, ep + d).wait_send()
        ck_copy(ep, ep + d).wait_send()

    each(1, n_ep - ep, sent_kv)
    pt_copy(x.at[0], x.at[1], 0).wait_send()
    pt_copy(mp_send, mp_recv, 1).wait_send()
    pt_copy(p_send, p_recv, 2).wait_send()

    each(1, n_ep, lambda d: res_copy(ep_peer(d), ep_peer(d)).wait_recv())
    c0 = comb_ref[...]
    c_hi = c0.astype(jnp.bfloat16)
    c1 = c0 - c_hi.astype(jnp.float32)
    c_mid = c1.astype(jnp.bfloat16)
    c_lo = (c1 - c_mid.astype(jnp.float32)).astype(jnp.bfloat16)
    back = ret[...].reshape(n_ep * SLOT, width)
    total = jnp.dot(c_hi, back, preferred_element_type=jnp.float32)
    total += jnp.dot(c_mid, back, preferred_element_type=jnp.float32)
    total += jnp.dot(c_lo, back, preferred_element_type=jnp.float32)
    eo_ref[...] = total.astype(jnp.bfloat16)
    each(1, n_ep, lambda d: res_copy(ep, ep_peer(d)).wait_send())


def route(expert_choice, route_weights, n_experts):
    flat_ids = expert_choice.reshape(-1)
    one_hot = (flat_ids[:, None] == jnp.arange(n_experts, dtype=jnp.int32)[None, :]).astype(
        jnp.int32
    )
    slot_rank = jnp.sum((jnp.cumsum(one_hot, axis=0) - one_hot) * one_hot, axis=1)
    slot_ids = (flat_ids * SLOT + slot_rank).reshape(expert_choice.shape)
    table = slot_ids[:, :, None] == jnp.arange(n_experts * SLOT, dtype=jnp.int32)[None, None, :]
    placing = jnp.sum(table.astype(jnp.bfloat16), axis=1)
    combine = jnp.sum(jnp.where(table, route_weights[:, :, None], 0.0), axis=1)
    return placing, combine


def local(
    n_ep,
    n_tp,
    queries,
    key_vectors,
    value_vectors,
    cumulative_gate,
    out_weight,
    expert_tokens,
    norm_gain,
    gate_weight,
    up_weight,
    down_weight,
    expert_choice,
    route_weights,
):
    tokens, width = expert_tokens.shape
    block, head = queries.shape
    units = gate_weight.shape[2]
    nz = n_tp // 2
    hops = nz // 2 - 1
    t_dev = block // n_tp
    col = width // n_ep
    bf16, f32 = jnp.bfloat16, jnp.float32

    tokens_float = expert_tokens.astype(f32)
    normed = (
        tokens_float
        * lax.rsqrt(jnp.mean(tokens_float * tokens_float, axis=1, keepdims=True) + eps_norm)
        * norm_gain
    ).astype(bf16)
    placing, combine = route(expert_choice, route_weights, n_ep)
    outgoing = (
        jnp.einsum("ts,td->sd", placing, normed, preferred_element_type=f32)
        .astype(bf16)
        .reshape(n_ep, SLOT, width)
    )
    kv = jnp.concatenate([key_vectors, value_vectors], axis=1)
    gate_tile = cumulative_gate.reshape(block // 128, 128)
    q_wide = jnp.pad(queries * bf16(1.0 / math.sqrt(head)), ((0, 0), (0, 128 - head)))

    dma = pltpu.SemaphoreType.DMA
    vmem = pltpu.VMEM
    mixer, experts = pl.pallas_call(
        functools.partial(body, n_ep, n_tp),
        out_shape=(
            jax.ShapeDtypeStruct((t_dev, width), bf16),
            jax.ShapeDtypeStruct((tokens, width), bf16),
        ),
        in_specs=[pl.BlockSpec(memory_space=vmem)] * 10,
        out_specs=(pl.BlockSpec(memory_space=vmem),) * 2,
        scratch_shapes=[
            vmem((n_ep, block, 128), bf16),
            vmem((n_ep, block // 128, 128), f32),
            vmem((2, hops, width, units), bf16),
            vmem((2, hops, width, units), bf16),
            vmem((2, hops, units, width), bf16),
            vmem((width, units), bf16),
            vmem((width, units), bf16),
            vmem((units, width), bf16),
            vmem((2, n_ep, SLOT, width), bf16),
            vmem((2, n_ep * SLOT, width), f32),
            vmem((n_ep * SLOT, width), bf16),
            vmem((n_ep * SLOT, width), bf16),
            vmem((n_ep, SLOT, width), bf16),
            vmem((n_ep, SLOT, width), bf16),
            vmem((nz, head, col), bf16),
            vmem((n_ep, nz, head, col), bf16),
            vmem((nz, t_dev, 128), bf16),
            vmem((nz, t_dev, 128), bf16),
            vmem((2 * t_dev, width), f32),
            vmem((t_dev, width), bf16),
            vmem((t_dev, width), bf16),
            vmem((block, 128), f32),
            vmem((block, 128), f32),
            vmem((block, 128), f32),
        ]
        + [dma((n_ep,))] * 8
        + [dma((nz,))] * 2
        + [dma((n_ep,))] * 2
        + [dma((nz,))] * 2
        + [dma((2, hops + 1, 3))] * 2
        + [dma((3,))] * 2,
        compiler_params=pltpu.CompilerParams(
            collective_id=0, has_side_effects=True, vmem_limit_bytes=63 * 2**20
        ),
        name="whole",
    )(
        q_wide,
        cumulative_gate,
        kv,
        gate_tile,
        gate_weight[0],
        up_weight[0],
        down_weight[0],
        out_weight,
        outgoing,
        combine,
    )
    return mixer, experts


def solution(mesh):
    placed = (
        P("ep", "tp"),
        P("ep", "tp"),
        P("ep", "tp"),
        P("ep", "tp"),
        P("tp", None),
        P(("ep", "tp"), None),
        P(),
        P("ep", None, "tp"),
        P("ep", None, "tp"),
        P("ep", "tp", None),
        P(("ep", "tp"), None),
        P(("ep", "tp"), None),
    )
    return jax.shard_map(
        functools.partial(local, mesh.shape["ep"], mesh.shape["tp"]),
        mesh=mesh,
        in_specs=placed,
        out_specs=(P(("ep", "tp"), None), P(("ep", "tp"), None)),
        check_vma=False,
    )
```

```python
import functools
import math

import jax
import jax.numpy as jnp
from jax import lax
from jax.experimental import pallas as pl
from jax.experimental.pallas import tpu as pltpu
from jax.sharding import PartitionSpec as P

SLOT = 16
TQ = 256
HEAD = 64
MESH = pl.DeviceIdType.MESH

eps_norm = 1e-05
clamp_limit = 7.0
sig_alpha = 1.702
floor_score = -1e30


def gate_row(tile):
    return jnp.concatenate([tile[r : r + 1, :] for r in range(tile.shape[0])], axis=1)


def activate(g, u):
    g = jnp.minimum(g, clamp_limit)
    u = jnp.clip(u, -clamp_limit, clamp_limit)
    return (g * jax.nn.sigmoid(sig_alpha * g) * (u + 1.0)).astype(jnp.bfloat16)


def attend_block(q_ref, cq_ref, kv_ref, ck_ref, m_ref, l_ref, acc_ref, diagonal):
    width = kv_ref.shape[0]
    tile = min(TQ, q_ref.shape[0])
    ck_row = gate_row(ck_ref[...])

    def one_tile(i, carry):
        rows = pl.ds(pl.multiple_of(i * tile, tile), tile)
        kv = kv_ref[...]
        s = lax.dot_general(
            q_ref[rows, :], kv, (((1,), (1,)), ((), ())), preferred_element_type=jnp.float32
        )
        s = s + (cq_ref[rows, :] - ck_row)
        if diagonal:
            q_pos = i * tile + lax.broadcasted_iota(jnp.int32, (tile, width), 0)
            k_pos = lax.broadcasted_iota(jnp.int32, (tile, width), 1)
            s = jnp.where(k_pos <= q_pos, s, floor_score)
        top = jnp.max(s, axis=1, keepdims=True)
        if diagonal:
            p = jnp.exp(s - top)
            m_ref[rows, :] = jnp.broadcast_to(top, (tile, 128))
            l_ref[rows, :] = jnp.broadcast_to(jnp.sum(p, axis=1, keepdims=True), (tile, 128))
            acc_ref[rows, :] = jnp.dot(
                p.astype(jnp.bfloat16), kv, preferred_element_type=jnp.float32
            )
        else:
            old = m_ref[rows, :]
            new = jnp.maximum(old, top)
            shrink = jnp.exp(old - new)
            p = jnp.exp(s - new[:, :1])
            m_ref[rows, :] = new
            l_ref[rows, :] = l_ref[rows, :] * shrink + jnp.sum(p, axis=1, keepdims=True)
            acc_ref[rows, :] = acc_ref[rows, :] * shrink + jnp.dot(
                p.astype(jnp.bfloat16), kv, preferred_element_type=jnp.float32
            )
        return carry

    lax.fori_loop(0, q_ref.shape[0] // tile, one_tile, 0)


N_BLOCKS = 4
DOWN_ORDER = {
    3: ((0, 0), (1, 0), (2, 0), (0, 1), (1, 1), (0, 2), (2, 1), (0, 3), (1, 2), (3, 0),
        (1, 3), (2, 2), (3, 1), (2, 3), (3, 2), (3, 3)),
    1: ((0, 0), (1, 0), (2, 0), (0, 1), (1, 1), (3, 0), (2, 1), (3, 1)),
}


def body(
    n_ep,
    n_tp,
    qt_ref,
    kt_ref,
    vt_ref,
    ck_ref,
    wg_ref,
    wu_ref,
    wd_ref,
    ow_ref,
    tok_ref,
    gain_ref,
    choice_ref,
    route_ref,
    mix_ref,
    eo_ref,
    q_ref,
    cq_ref,
    kv_ref,
    og_ref,
    comb_ref,
    kv_all,
    ck_all,
    rg,
    ru,
    lg,
    lu,
    dn,
    act,
    x,
    acc,
    p_send,
    p_recv,
    res,
    ret,
    osl,
    w_all,
    att_send,
    att_in,
    heads_ref,
    mix_acc,
    mp_send,
    mp_recv,
    m_ref,
    l_ref,
    att_acc,
    s_kv,
    r_kv,
    s_ck,
    r_ck,
    s_og,
    r_og,
    s_w,
    r_w,
    s_osl,
    r_osl,
    s_att,
    r_att,
    s_res,
    r_res,
    s_ring,
    r_ring,
    s_pt,
    r_pt,
):
    bf16, f32 = jnp.bfloat16, jnp.float32
    nz = n_tp // 2
    hops = nz // 2 - 1
    ep = lax.axis_index("ep")
    tp = lax.axis_index("tp")
    z = lax.div(tp, 2)
    core = lax.rem(tp, 2)
    right = lax.rem(tp + 2, n_tp)
    left = lax.rem(tp + n_tp - 2, n_tp)
    partner = tp + 1 - 2 * core
    units, width = wd_ref.shape
    block = q_ref.shape[0]
    tokens = tok_ref.shape[0]
    slots_all = n_ep * SLOT
    col = width // n_ep
    part = width // N_BLOCKS
    t_dev = mp_send.shape[0]

    def ep_peer(d):
        return lax.rem(ep + d, n_ep)

    def z_peer(d):
        return lax.rem(z + d, nz)

    def ep_copy(src, dst, send, recv, peer):
        return pltpu.make_async_remote_copy(
            src_ref=src, dst_ref=dst, send_sem=send, recv_sem=recv,
            device_id={"ep": peer}, device_id_type=MESH,
        )

    def tp_copy(src, dst, send, recv, peer):
        return pltpu.make_async_remote_copy(
            src_ref=src, dst_ref=dst, send_sem=send, recv_sem=recv,
            device_id={"tp": peer}, device_id_type=MESH,
        )

    def kv_copy(slot, peer):
        return ep_copy(kv_ref, kv_all.at[slot], s_kv.at[peer], r_kv.at[slot], peer)

    def ck_copy(slot, peer):
        return ep_copy(ck_ref, ck_all.at[slot], s_ck.at[peer], r_ck.at[slot], peer)

    def og_copy(slot, peer):
        return ep_copy(og_ref.at[peer], x.at[0, slot], s_og.at[peer], r_og.at[slot], peer)

    def res_copy(b, slot, peer):
        return ep_copy(
            res.at[b, peer], ret.at[b, slot], s_res.at[b, peer], r_res.at[b, slot], peer
        )

    def w_copy(slot, peer):
        return ep_copy(osl, w_all.at[slot], s_w.at[peer], r_w.at[slot], peer)

    my_cols = pl.ds(pl.multiple_of(ep * col, col), col)

    def osl_copy(slot, pz):
        return tp_copy(
            ow_ref.at[:, my_cols], osl.at[slot], s_osl.at[pz], r_osl.at[slot], 2 * pz + core
        )

    def att_copy(slot, pz):
        return tp_copy(
            att_send.at[pz], att_in.at[slot], s_att.at[pz], r_att.at[slot], 2 * pz + core
        )

    def pt_copy(src, dst, n):
        return tp_copy(src, dst, s_pt.at[n], r_pt.at[n], partner)

    def x_copy():
        return pt_copy(x.at[0], x.at[1], 0)

    def mp_copy():
        return pt_copy(mp_send, mp_recv, 1)

    def p_copy(b):
        return pt_copy(p_send.at[b], p_recv.at[b], 2 + b)

    peers = (right, left)
    own = (wg_ref, wu_ref)
    slots = (rg, ru)
    last = (lg, lu)
    firsts = 2 * hops + 1
    down_order = DOWN_ORDER[hops]
    items = firsts + len(down_order)

    def gu_copy(direction, h, j):
        a = j if direction == 0 else 1 - j
        n = 2 * h + j
        sems = (s_ring.at[direction, n], r_ring.at[direction, n])
        return lambda src, dst: tp_copy(src, dst, *sems, peers[direction]), a

    def gu_first(direction, j):
        make, a = gu_copy(direction, 0, j)
        return make(own[a], slots[a].at[direction, 0])

    def gu_next(direction, h, j):
        make, a = gu_copy(direction, h, j)
        return make(slots[a].at[direction, h - 1], slots[a].at[direction, h])

    def gu_last(direction):
        make, a = gu_copy(direction, hops, 0)
        return make(slots[a].at[direction, hops - 1], last[a])

    def down_copy(direction, i):
        b, h = down_order[i]
        cols = pl.ds(b * part, part)
        n = firsts + i
        rows = pl.ds(0, units)
        to = 1 + 2 * h + direction
        if h == hops:
            rows = pl.ds(direction * (units // 2), units // 2)
            to = 1 + 2 * hops
        if h == 0:
            src = wd_ref.at[rows, cols]
        else:
            src = dn.at[1 + 2 * (h - 1) + direction, rows, cols]
        return tp_copy(
            src, dn.at[to, rows, cols], s_ring.at[direction, n], r_ring.at[direction, n],
            peers[direction],
        )

    def start_down(i):
        for direction in range(2):
            down_copy(direction, i).start()

    def each(start, stop, fn):
        def run(d, carry):
            fn(d)
            return carry

        lax.fori_loop(start, stop, run, 0)

    barrier = pltpu.get_barrier_semaphore()
    each(
        1, n_ep,
        lambda d: pl.semaphore_signal(
            barrier, inc=1, device_id={"ep": ep_peer(d)}, device_id_type=MESH
        ),
    )
    each(
        1, nz,
        lambda d: pl.semaphore_signal(
            barrier, inc=1, device_id={"tp": 2 * z_peer(d) + core}, device_id_type=MESH
        ),
    )
    pl.semaphore_signal(barrier, inc=1, device_id={"tp": partner}, device_id_type=MESH)
    pl.semaphore_wait(barrier, n_ep - 1 + nz - 1 + 1)

    for j in range(2):
        for direction in range(2):
            gu_first(direction, j).start()
    each(1, nz, lambda d: osl_copy(z, z_peer(d)).start())

    kv_ref[...] = (
        jnp.concatenate([kt_ref[...].astype(f32), vt_ref[...].astype(f32)], axis=0)
        .T.astype(bf16)
    )
    scaled = qt_ref[...].astype(f32) * (1.0 / math.sqrt(HEAD))
    q_ref[...] = jnp.concatenate([scaled, jnp.zeros_like(scaled)], axis=0).T.astype(bf16)
    turned = ck_ref[...].T
    for r in range(block // 128):
        cq_ref[pl.ds(r * 128, 128), :] = turned[:, r : r + 1]

    ids = choice_ref[...]
    e_pos = lax.broadcasted_iota(jnp.int32, (n_ep, tokens), 0)
    named = [(e_pos == ids[k : k + 1, :]).astype(f32) for k in range(ids.shape[0])]
    both = functools.reduce(jnp.add, named)
    before = (
        lax.broadcasted_iota(jnp.int32, (tokens, tokens), 0)
        < lax.broadcasted_iota(jnp.int32, (tokens, tokens), 1)
    )
    earlier = jnp.dot(
        both.astype(bf16), before.astype(f32).astype(bf16), preferred_element_type=f32
    )
    s_pos = lax.broadcasted_iota(jnp.int32, (slots_all, tokens), 0).astype(f32)
    placing = jnp.zeros((slots_all, tokens), f32)
    comb = jnp.zeros((slots_all, tokens), f32)
    for k in range(ids.shape[0]):
        rank = jnp.sum(named[k] * earlier, axis=0, keepdims=True)
        slot = ids[k : k + 1, :].astype(f32) * SLOT + rank
        here = s_pos == slot
        placing = jnp.where(here, 1.0, placing)
        comb = jnp.where(here, route_ref[k : k + 1, :], comb)
    comb_ref[...] = comb.T
    tok = tok_ref[...].astype(f32)
    normed = (
        tok * lax.rsqrt(jnp.mean(tok * tok, axis=1, keepdims=True) + eps_norm) * gain_ref[...]
    ).astype(bf16)
    og_ref[...] = (
        jnp.dot(placing.astype(bf16), normed, preferred_element_type=f32)
        .astype(bf16)
        .reshape(n_ep, SLOT, width)
    )

    attend_block(q_ref, cq_ref, kv_ref, ck_ref, m_ref, l_ref, att_acc, True)

    def send_kv(d):
        kv_copy(ep, ep + d).start()
        ck_copy(ep, ep + d).start()

    near = jnp.minimum(n_ep - ep, 4)
    each(1, near, send_kv)
    each(1, n_ep, lambda d: og_copy(ep, ep_peer(d)).start())
    each(near, n_ep - ep, send_kv)
    x[0, ep] = og_ref[ep]
    osl[z] = ow_ref[:, my_cols]
    dn[0] = wd_ref[...]

    def attend_step(k):
        j = ep - k
        kv_copy(j, j).wait_recv()
        ck_copy(j, j).wait_recv()
        attend_block(q_ref, cq_ref, kv_all.at[j], ck_all.at[j], m_ref, l_ref, att_acc, False)

    def expert_units(g_ref, u_ref, n):
        cols = pl.ds(pl.multiple_of(n * units, units), units)
        for half in range(2):
            rows = x[half].reshape(slots_all, width)
            g = jnp.dot(rows, g_ref[...], preferred_element_type=f32)
            u = jnp.dot(rows, u_ref[...], preferred_element_type=f32)
            act[half, :, cols] = activate(g, u)

    per_step = -(-(n_ep - 1) // (2 * hops - 1))

    def hop_step(h, carry):
        for j in range(2):
            for direction in range(2):
                @pl.when(h == 0)
                def _():
                    gu_first(direction, j).wait_recv()

                @pl.when(h > 0)
                def _():
                    gu_next(direction, h, j).wait_recv()

                @pl.when(h < hops - 1)
                def _():
                    gu_next(direction, h + 1, j).start()

                if j == 0:
                    @pl.when(h == hops - 1)
                    def _():
                        gu_last(direction).start()

            if j == 1:
                @pl.when(h == hops - 1)
                def _():
                    for i in range(3):
                        start_down(i)

                @pl.when(h == 0)
                def _():
                    each(1, n_ep, lambda d: og_copy(ep_peer(d), ep_peer(d)).wait_recv())
                    x_copy().start()
                    each(1, nz, lambda d: osl_copy(z_peer(d), z_peer(d)).wait_recv())
                    each(1, n_ep, lambda d: w_copy(ep, ep_peer(d)).start())
                    w_all[ep] = osl[...]

            k0 = (2 * h + j) * per_step + 1
            each(k0, jnp.minimum(k0 + per_step, ep + 1), attend_step)

        @pl.when(h == 0)
        def _():
            x_copy().wait_recv()
            expert_units(wg_ref, wu_ref, 0)

        for direction in range(2):
            expert_units(rg.at[direction, h], ru.at[direction, h], 1 + 2 * h + direction)
        return carry

    lax.fori_loop(0, hops, hop_step, 0)

    for pz in range(nz):
        rows = pl.ds(pz * 2 * t_dev, 2 * t_dev)
        o = (att_acc[rows, :] / l_ref[rows, :])[:, HEAD:]
        att_send[pz] = jnp.concatenate([o[:t_dev], o[t_dev:]], axis=1).astype(bf16)
    for direction in range(2):
        gu_last(direction).wait_recv()
    each(1, nz, lambda d: att_copy(z, z_peer(d)).start())
    att_in[z] = att_send[z]
    expert_units(lg, lu, 1 + 2 * hops)

    def gather_heads():
        each(1, nz, lambda d: att_copy(z_peer(d), z_peer(d)).wait_recv())
        got = [att_in[pz].astype(f32) for pz in range(nz)]
        heads_ref[pl.ds(0, t_dev), :] = jnp.concatenate(
            [t[:, :HEAD] for t in got], axis=1
        ).astype(bf16)
        heads_ref[pl.ds(t_dev, t_dev), :] = jnp.concatenate(
            [t[:, HEAD:] for t in got], axis=1
        ).astype(bf16)
        each(1, n_ep, lambda d: w_copy(ep_peer(d), ep_peer(d)).wait_recv())

    def project(e):
        piece = w_all[e].reshape(nz * HEAD, col)
        mix_acc[:, pl.ds(pl.multiple_of(e * col, col), col)] = jnp.dot(
            heads_ref[...], piece, preferred_element_type=f32
        )

    theirs = pl.ds(pl.multiple_of((1 - core) * t_dev, t_dev), t_dev)
    mine = pl.ds(pl.multiple_of(core * t_dev, t_dev), t_dev)

    def send_mix():
        mp_send[...] = mix_acc[theirs, :].astype(bf16)
        mp_copy().start()

    def take_mix():
        mp_copy().wait_recv()
        mix_ref[...] = (mix_acc[mine, :] + mp_recv[...].astype(f32)).astype(bf16)

    def finish_units(b):
        weights = dn[:, :, b * part : (b + 1) * part].reshape(nz * units, part)
        p_send[b] = jnp.dot(act[1], weights, preferred_element_type=f32).astype(bf16)
        p_copy(b).start()
        acc[b] = jnp.dot(act[0], weights, preferred_element_type=f32)

    def send_home(b):
        p_copy(b).wait_recv()
        res[b] = (acc[b] + p_recv[b].astype(f32)).astype(bf16).reshape(n_ep, SLOT, part)
        each(1, n_ep, lambda d: res_copy(b, ep, ep_peer(d)).start())
        ret[b, ep] = res[b, ep]

    c0 = comb_ref[...]
    c_hi = c0.astype(bf16)
    c1 = c0 - c_hi.astype(f32)
    c_mid = c1.astype(bf16)
    c_lo = (c1 - c_mid.astype(f32)).astype(bf16)

    def combine(b):
        each(1, n_ep, lambda d: res_copy(b, ep_peer(d), ep_peer(d)).wait_recv())
        back = ret[b].reshape(slots_all, part)
        total = jnp.dot(c_hi, back, preferred_element_type=f32)
        total += jnp.dot(c_mid, back, preferred_element_type=f32)
        total += jnp.dot(c_lo, back, preferred_element_type=f32)
        eo_ref[:, b * part : (b + 1) * part] = total.astype(bf16)

    count = len(down_order)
    issued = 3
    arrived = []
    pending = []
    mixer_work = [gather_heads]
    quarter = -(-n_ep // 4)
    for q in range(4):
        mixer_work.append(
            functools.partial(each, q * quarter, min((q + 1) * quarter, n_ep), project)
        )
    mixer_work += [send_mix, take_mix]
    mixer_at = min(4, count - 8) if count > 8 else 0
    for i in range(count):
        for direction in range(2):
            down_copy(direction, i).wait_recv()
        arrived.append(down_order[i])
        while issued < min(count, i + 3):
            b, h = down_order[issued]
            if h > 0 and (b, h - 1) not in arrived:
                break
            start_down(issued)
            issued += 1
        for b in pending:
            send_home(b)
        pending = []
        b, h = down_order[i]
        if h == hops:
            finish_units(b)
            pending.append(b)
        elif i >= mixer_at and mixer_work:
            mixer_work.pop(0)()
    for b in pending:
        send_home(b)
    for work in mixer_work:
        work()

    each(1, nz, lambda d: osl_copy(z, z_peer(d)).wait_send())
    each(1, nz, lambda d: att_copy(z, z_peer(d)).wait_send())
    for direction in range(2):
        for j in range(2):
            gu_first(direction, j).wait_send()
            each(1, hops, lambda h: gu_next(direction, h, j).wait_send())
        gu_last(direction).wait_send()
        for i in range(count):
            down_copy(direction, i).wait_send()
    each(1, n_ep, lambda d: og_copy(ep, ep_peer(d)).wait_send())
    each(1, n_ep, lambda d: w_copy(ep, ep_peer(d)).wait_send())

    def sent_kv(d):
        kv_copy(ep, ep + d).wait_send()
        ck_copy(ep, ep + d).wait_send()

    each(1, n_ep - ep, sent_kv)
    x_copy().wait_send()
    mp_copy().wait_send()
    for b in range(N_BLOCKS):
        p_copy(b).wait_send()
    for b in range(N_BLOCKS):
        combine(b)
    for b in range(N_BLOCKS):
        each(1, n_ep, lambda d: res_copy(b, ep, ep_peer(d)).wait_send())


def local(
    n_ep,
    n_tp,
    queries,
    key_vectors,
    value_vectors,
    cumulative_gate,
    out_weight,
    expert_tokens,
    norm_gain,
    gate_weight,
    up_weight,
    down_weight,
    expert_choice,
    route_weights,
):
    tokens, width = expert_tokens.shape
    block, head = queries.shape
    units = gate_weight.shape[2]
    nz = n_tp // 2
    hops = nz // 2 - 1
    t_dev = block // n_tp
    col = width // n_ep
    part = width // N_BLOCKS
    slots_all = n_ep * SLOT
    items = 2 * hops + 1 + len(DOWN_ORDER[hops])
    bf16, f32 = jnp.bfloat16, jnp.float32
    dma = pltpu.SemaphoreType.DMA
    vmem = pltpu.VMEM
    return pl.pallas_call(
        functools.partial(body, n_ep, n_tp),
        out_shape=(
            jax.ShapeDtypeStruct((t_dev, width), bf16),
            jax.ShapeDtypeStruct((tokens, width), bf16),
        ),
        in_specs=[pl.BlockSpec(memory_space=vmem)] * 12,
        out_specs=(pl.BlockSpec(memory_space=vmem),) * 2,
        scratch_shapes=[
            vmem((block, 128), bf16),
            vmem((block, 1), f32),
            vmem((block, 128), bf16),
            vmem((n_ep, SLOT, width), bf16),
            vmem((tokens, slots_all), f32),
            vmem((n_ep, block, 128), bf16),
            vmem((n_ep, block // 128, 128), f32),
            vmem((2, hops, width, units), bf16),
            vmem((2, hops, width, units), bf16),
            vmem((width, units), bf16),
            vmem((width, units), bf16),
            vmem((nz, units, width), bf16),
            vmem((2, slots_all, nz * units), bf16),
            vmem((2, n_ep, SLOT, width), bf16),
            vmem((N_BLOCKS, slots_all, part), f32),
            vmem((N_BLOCKS, slots_all, part), bf16),
            vmem((N_BLOCKS, slots_all, part), bf16),
            vmem((N_BLOCKS, n_ep, SLOT, part), bf16),
            vmem((N_BLOCKS, n_ep, SLOT, part), bf16),
            vmem((nz, head, col), bf16),
            vmem((n_ep, nz, head, col), bf16),
            vmem((nz, t_dev, 128), bf16),
            vmem((nz, t_dev, 128), bf16),
            vmem((2 * t_dev, nz * head), bf16),
            vmem((2 * t_dev, width), f32),
            vmem((t_dev, width), bf16),
            vmem((t_dev, width), bf16),
            vmem((block, 128), f32),
            vmem((block, 128), f32),
            vmem((block, 128), f32),
        ]
        + [dma((n_ep,))] * 8
        + [dma((nz,))] * 4
        + [dma((N_BLOCKS, n_ep))] * 2
        + [dma((2, items))] * 2
        + [dma((2 + N_BLOCKS,))] * 2,
        compiler_params=pltpu.CompilerParams(
            collective_id=0, has_side_effects=True, vmem_limit_bytes=60 * 2**20
        ),
        name="whole",
    )(
        queries.T,
        key_vectors.T,
        value_vectors.T,
        cumulative_gate.reshape(block // 128, 128),
        gate_weight[0],
        up_weight[0],
        down_weight[0],
        out_weight,
        expert_tokens,
        norm_gain.reshape(1, width),
        expert_choice.T,
        route_weights.T,
    )


def solution(mesh):
    placed = (
        P("ep", "tp"),
        P("ep", "tp"),
        P("ep", "tp"),
        P("ep", "tp"),
        P("tp", None),
        P(("ep", "tp"), None),
        P(),
        P("ep", None, "tp"),
        P("ep", None, "tp"),
        P("ep", "tp", None),
        P(("ep", "tp"), None),
        P(("ep", "tp"), None),
    )
    return jax.shard_map(
        functools.partial(local, mesh.shape["ep"], mesh.shape["tp"]),
        mesh=mesh,
        in_specs=placed,
        out_specs=(P(("ep", "tp"), None), P(("ep", "tp"), None)),
        check_vma=False,
    )
```

```python
import functools
import math

import jax
import jax.numpy as jnp
from jax import lax
from jax.experimental import pallas as pl
from jax.experimental.pallas import tpu as pltpu
from jax.sharding import PartitionSpec as P

SLOT = 16
SIDE = 4
HEAD = 64
MESH = pl.DeviceIdType.MESH

eps_norm = 1e-05
clamp_limit = 7.0
sig_alpha = 1.702
floor_score = -1e30


def gate_row(tile):
    return jnp.concatenate([tile[r : r + 1, :] for r in range(tile.shape[0])], axis=1)


def activate(g, u):
    g = jnp.minimum(g, clamp_limit)
    u = jnp.clip(u, -clamp_limit, clamp_limit)
    return (g * jax.nn.sigmoid(sig_alpha * g) * (u + 1.0)).astype(jnp.bfloat16)


def attend_block(q_ref, cq_ref, kv_ref, ck_ref, m_ref, l_ref, acc_ref, diagonal):
    tile = q_ref.shape[0] // 2
    ck_all_row = gate_row(ck_ref[...])
    for i in range(2):
        rows = pl.ds(i * tile, tile)
        width = (i + 1) * tile if diagonal else kv_ref.shape[0]
        kv = kv_ref[:width, :]
        ck_row = ck_all_row[:, :width]
        s = lax.dot_general(
            q_ref[rows, :], kv, (((1,), (1,)), ((), ())), preferred_element_type=jnp.float32
        )
        s = s + (cq_ref[rows, :] - ck_row)
        if diagonal:
            q_pos = i * tile + lax.broadcasted_iota(jnp.int32, (tile, width), 0)
            k_pos = lax.broadcasted_iota(jnp.int32, (tile, width), 1)
            s = jnp.where(k_pos <= q_pos, s, floor_score)
        top = jnp.max(s, axis=1, keepdims=True)
        if diagonal:
            p = jnp.exp(s - top)
            m_ref[rows, :] = jnp.broadcast_to(top, (tile, 128))
            l_ref[rows, :] = jnp.broadcast_to(jnp.sum(p, axis=1, keepdims=True), (tile, 128))
            acc_ref[rows, :] = jnp.dot(
                p.astype(jnp.bfloat16), kv, preferred_element_type=jnp.float32
            )
        else:
            old = m_ref[rows, :]
            new = jnp.maximum(old, top)
            shrink = jnp.exp(old - new)
            p = jnp.exp(s - new[:, :1])
            m_ref[rows, :] = new
            l_ref[rows, :] = l_ref[rows, :] * shrink + jnp.sum(p, axis=1, keepdims=True)
            acc_ref[rows, :] = acc_ref[rows, :] * shrink + jnp.dot(
                p.astype(jnp.bfloat16), kv, preferred_element_type=jnp.float32
            )


N_BLOCKS = 4
DOWN_ORDER = {
    3: ((0, 0), (1, 0), (2, 0), (0, 1), (1, 1), (0, 2), (2, 1), (0, 3), (1, 2), (3, 0),
        (1, 3), (2, 2), (3, 1), (2, 3), (3, 2), (3, 3)),
    1: ((0, 0), (1, 0), (2, 0), (0, 1), (1, 1), (3, 0), (2, 1), (3, 1)),
}


def body(
    n_ep,
    n_tp,
    qt_ref,
    kt_ref,
    vt_ref,
    ck_ref,
    wg_ref,
    wu_ref,
    wd_ref,
    ow_ref,
    tok_ref,
    gain_ref,
    choice_ref,
    route_ref,
    mix_ref,
    eo_ref,
    q_ref,
    cq_ref,
    og_ref,
    comb_ref,
    kv_all,
    ck_all,
    rg,
    ru,
    lg,
    lu,
    dn,
    act,
    x,
    acc,
    p_send,
    p_recv,
    res,
    ret,
    w_all,
    att_send,
    att_in,
    heads_ref,
    mix_acc,
    mp_send,
    mp_recv,
    m_ref,
    l_ref,
    att_acc,
    s_kv,
    r_kv,
    s_ck,
    r_ck,
    s_og,
    r_og,
    s_w,
    r_w,
    s_osl,
    r_osl,
    s_att,
    r_att,
    s_res,
    r_res,
    s_ring,
    r_ring,
    s_pt,
    r_pt,
):
    bf16, f32 = jnp.bfloat16, jnp.float32
    nz = n_tp // 2
    hops = nz // 2 - 1
    ep = lax.axis_index("ep")
    tp = lax.axis_index("tp")
    z = lax.div(tp, 2)
    core = lax.rem(tp, 2)
    right = lax.rem(tp + 2, n_tp)
    left = lax.rem(tp + n_tp - 2, n_tp)
    partner = tp + 1 - 2 * core
    units, width = wd_ref.shape
    block = q_ref.shape[0]
    tokens = tok_ref.shape[0]
    slots_all = n_ep * SLOT
    col = width // n_ep
    part = width // N_BLOCKS
    t_dev = mp_send.shape[0]

    def ep_peer(d):
        return lax.rem(ep + d, n_ep)

    def z_peer(d):
        return lax.rem(z + d, nz)

    def ep_copy(src, dst, send, recv, peer):
        return pltpu.make_async_remote_copy(
            src_ref=src, dst_ref=dst, send_sem=send, recv_sem=recv,
            device_id={"ep": peer}, device_id_type=MESH,
        )

    def tp_copy(src, dst, send, recv, peer):
        return pltpu.make_async_remote_copy(
            src_ref=src, dst_ref=dst, send_sem=send, recv_sem=recv,
            device_id={"tp": peer}, device_id_type=MESH,
        )

    y = lax.div(ep, SIDE)
    x_at = lax.rem(ep, SIDE)
    x_next = y * SIDE + lax.rem(x_at + 1, SIDE)
    x_prev = y * SIDE + lax.rem(x_at + SIDE - 1, SIDE)
    x_far = y * SIDE + lax.rem(x_at + 2, SIDE)
    y_next = lax.rem(y + 1, SIDE)
    y_prev = lax.rem(y + SIDE - 1, SIDE)
    y_far = lax.rem(y + 2, SIDE)

    class Spread:
        def __init__(self, buf, send, recv):
            self.buf, self.send, self.recv = buf, send, recv
            self.half = buf.shape[1] // 2

        def move(self, n, region, peer):
            return ep_copy(region, region, self.send.at[n], self.recv.at[n], peer)

        def part(self, slot, n):
            return self.buf.at[slot, pl.ds(n * self.half, self.half)]

        def rows(self, row, n, count):
            return self.buf.at[pl.ds(row * SIDE + n, count)]

        def sent(self, step):
            if step == 1:
                return (
                    self.move(0, self.buf.at[ep], x_next),
                    self.move(1, self.buf.at[ep], x_prev),
                )
            if step == 2:
                return (
                    self.move(2, self.part(x_prev, 0), x_next),
                    self.move(3, self.part(x_next, 1), x_prev),
                )
            up, down = y_next * SIDE + x_at, y_prev * SIDE + x_at
            if step == 3:
                return (
                    self.move(4, self.rows(y, 0, SIDE), up),
                    self.move(5, self.rows(y, 0, SIDE), down),
                )
            return (
                self.move(6, self.rows(y_prev, 0, SIDE // 2), up),
                self.move(7, self.rows(y_next, SIDE // 2, SIDE // 2), down),
            )

        def come(self, step):
            if step == 1:
                return (
                    self.move(0, self.buf.at[x_prev], x_next),
                    self.move(1, self.buf.at[x_next], x_prev),
                )
            if step == 2:
                return (
                    self.move(2, self.part(x_far, 0), x_next),
                    self.move(3, self.part(x_far, 1), x_prev),
                )
            up, down = y_next * SIDE + x_at, y_prev * SIDE + x_at
            if step == 3:
                return (
                    self.move(4, self.rows(y_prev, 0, SIDE), up),
                    self.move(5, self.rows(y_next, 0, SIDE), down),
                )
            return (
                self.move(6, self.rows(y_far, 0, SIDE // 2), up),
                self.move(7, self.rows(y_far, SIDE // 2, SIDE // 2), down),
            )

        def wait(self, step):
            for copy in self.come(step):
                copy.wait_recv()

        def start(self, step):
            for copy in self.sent(step):
                copy.start()

        def done(self):
            for step in range(1, 5):
                for copy in self.sent(step):
                    copy.wait_send()

    kv_spread = Spread(kv_all, s_kv, r_kv)
    w_spread = Spread(w_all, s_w, r_w)

    def ck_copy(slot, peer):
        return ep_copy(ck_ref, ck_all.at[slot], s_ck.at[peer], r_ck.at[slot], peer)

    def og_copy(slot, peer):
        return ep_copy(og_ref.at[peer], x.at[0, slot], s_og.at[peer], r_og.at[slot], peer)

    def res_copy(b, slot, peer):
        return ep_copy(
            res.at[b, peer], ret.at[b, slot], s_res.at[b, peer], r_res.at[b, slot], peer
        )

    my_cols = pl.ds(pl.multiple_of(ep * col, col), col)

    def osl_copy(slot, pz):
        return tp_copy(
            ow_ref.at[:, my_cols], w_all.at[ep, slot], s_osl.at[pz], r_osl.at[slot], 2 * pz + core
        )

    def att_copy(slot, pz):
        return tp_copy(
            att_send.at[pz], att_in.at[slot], s_att.at[pz], r_att.at[slot], 2 * pz + core
        )

    def pt_copy(src, dst, n):
        return tp_copy(src, dst, s_pt.at[n], r_pt.at[n], partner)

    def x_copy():
        return pt_copy(x.at[0], x.at[1], 0)

    def mp_copy():
        return pt_copy(mp_send, mp_recv, 1)

    def p_copy(b):
        return pt_copy(p_send.at[b], p_recv.at[b], 2 + b)

    peers = (right, left)
    own = (wg_ref, wu_ref)
    slots = (rg, ru)
    last = (lg, lu)
    firsts = 2 * hops + 1
    down_order = DOWN_ORDER[hops]
    items = firsts + len(down_order)

    def gu_copy(direction, h, j):
        a = j if direction == 0 else 1 - j
        n = 2 * h + j
        sems = (s_ring.at[direction, n], r_ring.at[direction, n])
        return lambda src, dst: tp_copy(src, dst, *sems, peers[direction]), a

    def gu_first(direction, j):
        make, a = gu_copy(direction, 0, j)
        return make(own[a], slots[a].at[direction, 0])

    def gu_next(direction, h, j):
        make, a = gu_copy(direction, h, j)
        return make(slots[a].at[direction, h - 1], slots[a].at[direction, h])

    def gu_last(direction):
        make, a = gu_copy(direction, hops, 0)
        return make(slots[a].at[direction, hops - 1], last[a])

    def down_copy(direction, i):
        b, h = down_order[i]
        cols = pl.ds(b * part, part)
        n = firsts + i
        rows = pl.ds(0, units)
        to = 1 + 2 * h + direction
        if h == hops:
            rows = pl.ds(direction * (units // 2), units // 2)
            to = 1 + 2 * hops
        if h == 0:
            src = wd_ref.at[rows, cols]
        else:
            src = dn.at[1 + 2 * (h - 1) + direction, rows, cols]
        return tp_copy(
            src, dn.at[to, rows, cols], s_ring.at[direction, n], r_ring.at[direction, n],
            peers[direction],
        )

    def start_down(i):
        for direction in range(2):
            down_copy(direction, i).start()

    def each(start, stop, fn):
        def run(d, carry):
            fn(d)
            return carry

        lax.fori_loop(start, stop, run, 0)

    barrier = pltpu.get_barrier_semaphore()
    each(
        1, n_ep,
        lambda d: pl.semaphore_signal(
            barrier, inc=1, device_id={"ep": ep_peer(d)}, device_id_type=MESH
        ),
    )
    each(
        1, nz,
        lambda d: pl.semaphore_signal(
            barrier, inc=1, device_id={"tp": 2 * z_peer(d) + core}, device_id_type=MESH
        ),
    )
    pl.semaphore_signal(barrier, inc=1, device_id={"tp": partner}, device_id_type=MESH)
    pl.semaphore_wait(barrier, n_ep - 1 + nz - 1 + 1)

    for j in range(2):
        for direction in range(2):
            gu_first(direction, j).start()
    each(1, nz, lambda d: osl_copy(z, z_peer(d)).start())

    kv_all[ep] = (
        jnp.concatenate([kt_ref[...].astype(f32), vt_ref[...].astype(f32)], axis=0)
        .T.astype(bf16)
    )
    scaled = qt_ref[...].astype(f32) * (1.0 / math.sqrt(HEAD))
    q_ref[...] = jnp.concatenate([scaled, jnp.zeros_like(scaled)], axis=0).T.astype(bf16)
    turned = ck_ref[...].T
    for r in range(block // 128):
        cq_ref[pl.ds(r * 128, 128), :] = turned[:, r : r + 1]

    ids = choice_ref[...]
    e_pos = lax.broadcasted_iota(jnp.int32, (n_ep, tokens), 0)
    named = [(e_pos == ids[k : k + 1, :]).astype(f32) for k in range(ids.shape[0])]
    both = functools.reduce(jnp.add, named)
    before = (
        lax.broadcasted_iota(jnp.int32, (tokens, tokens), 0)
        < lax.broadcasted_iota(jnp.int32, (tokens, tokens), 1)
    )
    earlier = jnp.dot(
        both.astype(bf16), before.astype(f32).astype(bf16), preferred_element_type=f32
    )
    s_pos = lax.broadcasted_iota(jnp.int32, (slots_all, tokens), 0).astype(f32)
    placing = jnp.zeros((slots_all, tokens), f32)
    comb = jnp.zeros((slots_all, tokens), f32)
    for k in range(ids.shape[0]):
        rank = jnp.sum(named[k] * earlier, axis=0, keepdims=True)
        slot = ids[k : k + 1, :].astype(f32) * SLOT + rank
        here = s_pos == slot
        placing = jnp.where(here, 1.0, placing)
        comb = jnp.where(here, route_ref[k : k + 1, :], comb)
    comb_ref[...] = comb.T
    tok = tok_ref[...].astype(f32)
    normed = (
        tok * lax.rsqrt(jnp.mean(tok * tok, axis=1, keepdims=True) + eps_norm) * gain_ref[...]
    ).astype(bf16)
    og_ref[...] = (
        jnp.dot(placing.astype(bf16), normed, preferred_element_type=f32)
        .astype(bf16)
        .reshape(n_ep, SLOT, width)
    )

    attend_block(q_ref, cq_ref, kv_all.at[ep], ck_ref, m_ref, l_ref, att_acc, True)

    kv_spread.start(1)
    each(1, n_ep - ep, lambda d: ck_copy(ep, ep + d).start())
    each(1, n_ep, lambda d: og_copy(ep, ep_peer(d)).start())
    x[0, ep] = og_ref[ep]
    w_all[ep, z] = ow_ref[:, my_cols]
    dn[0] = wd_ref[...]

    def attend_step(j):
        ck_copy(j, j).wait_recv()
        attend_block(q_ref, cq_ref, kv_all.at[j], ck_all.at[j], m_ref, l_ref, att_acc, False)

    def expert_units(g_ref, u_ref, n):
        cols = pl.ds(pl.multiple_of(n * units, units), units)
        for half in range(2):
            rows = x[half].reshape(slots_all, width)
            g = jnp.dot(rows, g_ref[...], preferred_element_type=f32)
            u = jnp.dot(rows, u_ref[...], preferred_element_type=f32)
            act[half, :, cols] = activate(g, u)

    def units_of(h):
        for direction in range(2):
            expert_units(rg.at[direction, h], ru.at[direction, h], 1 + 2 * h + direction)

    def kv_step(step):
        kv_spread.wait(step - 1)
        kv_spread.start(step)

    def w_step(step):
        w_spread.wait(step - 1)
        w_spread.start(step)

    def first_w():
        each(1, nz, lambda d: osl_copy(z_peer(d), z_peer(d)).wait_recv())
        w_spread.start(1)

    def swap_rows():
        each(1, n_ep, lambda d: og_copy(ep_peer(d), ep_peer(d)).wait_recv())
        x_copy().start()

    def own_units():
        x_copy().wait_recv()
        expert_units(wg_ref, wu_ref, 0)

    def send_attention():
        for pz in range(nz):
            rows = pl.ds(pz * 2 * t_dev, 2 * t_dev)
            o = (att_acc[rows, :] / l_ref[rows, :])[:, HEAD:]
            att_send[pz] = jnp.concatenate([o[:t_dev], o[t_dev:]], axis=1).astype(bf16)
        att_in[z] = att_send[z]

    def above(n):
        return SIDE * jnp.maximum(y - n, 0)

    def units_safe(h):
        if h < hops:
            units_of(h)

    work_list = [
        (0, lambda: kv_step(2)),
        (0, first_w),
        (1, lambda: kv_step(3)),
        (1, swap_rows),
        (1, lambda: each(SIDE * y, ep, attend_step)),
        (1, lambda: w_step(2)),
        (2, own_units),
        (2, lambda: units_safe(0)),
        (3, lambda: kv_step(4)),
        (3, lambda: each(above(1), SIDE * y, attend_step)),
        (4, lambda: w_step(3)),
        (4, lambda: units_safe(1)),
        (4, lambda: each(0, above(2), attend_step)),
        (5, lambda: kv_spread.wait(4)),
        (5, lambda: each(above(2), above(1), attend_step)),
        (6, send_attention),
        (6, lambda: w_step(4)),
        (6, lambda: units_safe(2)),
    ]
    for n in range(firsts):
        h, j = n // 2, n % 2
        for direction in range(2):
            if n == firsts - 1:
                gu_last(direction).wait_recv()
            elif h == 0:
                gu_first(direction, j).wait_recv()
            else:
                gu_next(direction, h, j).wait_recv()
            follow = n + 2
            if follow < firsts - 1:
                gu_next(direction, h + 1, j).start()
            elif follow == firsts - 1:
                gu_last(direction).start()
        if n == firsts - 2:
            for i in range(3):
                start_down(i)
        for at, work in work_list:
            if min(at, firsts - 1) == n:
                work()
    each(1, nz, lambda d: att_copy(z, z_peer(d)).start())
    expert_units(lg, lu, 1 + 2 * hops)

    def gather_heads():
        each(1, nz, lambda d: att_copy(z_peer(d), z_peer(d)).wait_recv())
        got = [att_in[pz].astype(f32) for pz in range(nz)]
        heads_ref[pl.ds(0, t_dev), :] = jnp.concatenate(
            [t[:, :HEAD] for t in got], axis=1
        ).astype(bf16)
        heads_ref[pl.ds(t_dev, t_dev), :] = jnp.concatenate(
            [t[:, HEAD:] for t in got], axis=1
        ).astype(bf16)
        w_spread.wait(4)

    def project(e):
        piece = w_all[e].reshape(nz * HEAD, col)
        mix_acc[:, pl.ds(pl.multiple_of(e * col, col), col)] = jnp.dot(
            heads_ref[...], piece, preferred_element_type=f32
        )

    theirs = pl.ds(pl.multiple_of((1 - core) * t_dev, t_dev), t_dev)
    mine = pl.ds(pl.multiple_of(core * t_dev, t_dev), t_dev)

    def send_mix():
        mp_send[...] = mix_acc[theirs, :].astype(bf16)
        mp_copy().start()

    def take_mix():
        mp_copy().wait_recv()
        mix_ref[...] = (mix_acc[mine, :] + mp_recv[...].astype(f32)).astype(bf16)

    def finish_units(b):
        weights = dn[:, :, b * part : (b + 1) * part].reshape(nz * units, part)
        p_send[b] = jnp.dot(act[1], weights, preferred_element_type=f32).astype(bf16)
        p_copy(b).start()
        acc[b] = jnp.dot(act[0], weights, preferred_element_type=f32)

    def send_home(b):
        p_copy(b).wait_recv()
        res[b] = (acc[b] + p_recv[b].astype(f32)).astype(bf16).reshape(n_ep, SLOT, part)
        each(1, n_ep, lambda d: res_copy(b, ep, ep_peer(d)).start())
        ret[b, ep] = res[b, ep]

    c0 = comb_ref[...]
    c_hi = c0.astype(bf16)
    c1 = c0 - c_hi.astype(f32)
    c_mid = c1.astype(bf16)
    c_lo = (c1 - c_mid.astype(f32)).astype(bf16)

    def combine(b):
        each(1, n_ep, lambda d: res_copy(b, ep_peer(d), ep_peer(d)).wait_recv())
        back = ret[b].reshape(slots_all, part)
        total = jnp.dot(c_hi, back, preferred_element_type=f32)
        total += jnp.dot(c_mid, back, preferred_element_type=f32)
        total += jnp.dot(c_lo, back, preferred_element_type=f32)
        eo_ref[:, b * part : (b + 1) * part] = total.astype(bf16)

    count = len(down_order)
    issued = 3
    arrived = []
    pending = []
    mixer_work = [gather_heads]
    quarter = -(-n_ep // 4)
    for q in range(4):
        mixer_work.append(
            functools.partial(each, q * quarter, min((q + 1) * quarter, n_ep), project)
        )
    mixer_work += [send_mix, take_mix]
    mixer_at = min(4, count - 8) if count > 8 else 0
    for i in range(count):
        for direction in range(2):
            down_copy(direction, i).wait_recv()
        arrived.append(down_order[i])
        while issued < min(count, i + 3):
            b, h = down_order[issued]
            if h > 0 and (b, h - 1) not in arrived:
                break
            start_down(issued)
            issued += 1
        for b in pending:
            send_home(b)
        pending = []
        b, h = down_order[i]
        if h == hops:
            finish_units(b)
            pending.append(b)
        elif i >= mixer_at and mixer_work:
            mixer_work.pop(0)()
    for b in pending:
        send_home(b)
    for work in mixer_work:
        work()

    each(1, nz, lambda d: osl_copy(z, z_peer(d)).wait_send())
    each(1, nz, lambda d: att_copy(z, z_peer(d)).wait_send())
    for direction in range(2):
        for j in range(2):
            gu_first(direction, j).wait_send()
            each(1, hops, lambda h: gu_next(direction, h, j).wait_send())
        gu_last(direction).wait_send()
        for i in range(count):
            down_copy(direction, i).wait_send()
    each(1, n_ep, lambda d: og_copy(ep, ep_peer(d)).wait_send())
    kv_spread.done()
    w_spread.done()
    each(1, n_ep - ep, lambda d: ck_copy(ep, ep + d).wait_send())
    x_copy().wait_send()
    mp_copy().wait_send()
    for b in range(N_BLOCKS):
        p_copy(b).wait_send()
    for b in range(N_BLOCKS):
        combine(b)
    for b in range(N_BLOCKS):
        each(1, n_ep, lambda d: res_copy(b, ep, ep_peer(d)).wait_send())


def local(
    n_ep,
    n_tp,
    queries,
    key_vectors,
    value_vectors,
    cumulative_gate,
    out_weight,
    expert_tokens,
    norm_gain,
    gate_weight,
    up_weight,
    down_weight,
    expert_choice,
    route_weights,
):
    tokens, width = expert_tokens.shape
    block, head = queries.shape
    units = gate_weight.shape[2]
    nz = n_tp // 2
    hops = nz // 2 - 1
    t_dev = block // n_tp
    col = width // n_ep
    part = width // N_BLOCKS
    slots_all = n_ep * SLOT
    items = 2 * hops + 1 + len(DOWN_ORDER[hops])
    bf16, f32 = jnp.bfloat16, jnp.float32
    dma = pltpu.SemaphoreType.DMA
    vmem = pltpu.VMEM
    return pl.pallas_call(
        functools.partial(body, n_ep, n_tp),
        out_shape=(
            jax.ShapeDtypeStruct((t_dev, width), bf16),
            jax.ShapeDtypeStruct((tokens, width), bf16),
        ),
        in_specs=[pl.BlockSpec(memory_space=vmem)] * 12,
        out_specs=(pl.BlockSpec(memory_space=vmem),) * 2,
        scratch_shapes=[
            vmem((block, 128), bf16),
            vmem((block, 1), f32),
            vmem((n_ep, SLOT, width), bf16),
            vmem((tokens, slots_all), f32),
            vmem((n_ep, block, 128), bf16),
            vmem((n_ep, block // 128, 128), f32),
            vmem((2, hops, width, units), bf16),
            vmem((2, hops, width, units), bf16),
            vmem((width, units), bf16),
            vmem((width, units), bf16),
            vmem((nz, units, width), bf16),
            vmem((2, slots_all, nz * units), bf16),
            vmem((2, n_ep, SLOT, width), bf16),
            vmem((N_BLOCKS, slots_all, part), f32),
            vmem((N_BLOCKS, slots_all, part), bf16),
            vmem((N_BLOCKS, slots_all, part), bf16),
            vmem((N_BLOCKS, n_ep, SLOT, part), bf16),
            vmem((N_BLOCKS, n_ep, SLOT, part), bf16),
            vmem((n_ep, nz, head, col), bf16),
            vmem((nz, t_dev, 128), bf16),
            vmem((nz, t_dev, 128), bf16),
            vmem((2 * t_dev, nz * head), bf16),
            vmem((2 * t_dev, width), f32),
            vmem((t_dev, width), bf16),
            vmem((t_dev, width), bf16),
            vmem((block, 128), f32),
            vmem((block, 128), f32),
            vmem((block, 128), f32),
        ]
        + [dma((8,))] * 2
        + [dma((n_ep,))] * 4
        + [dma((8,))] * 2
        + [dma((nz,))] * 4
        + [dma((N_BLOCKS, n_ep))] * 2
        + [dma((2, items))] * 2
        + [dma((2 + N_BLOCKS,))] * 2,
        compiler_params=pltpu.CompilerParams(
            collective_id=0, has_side_effects=True, vmem_limit_bytes=60 * 2**20
        ),
        name="whole",
    )(
        queries.T,
        key_vectors.T,
        value_vectors.T,
        cumulative_gate.reshape(block // 128, 128),
        gate_weight[0],
        up_weight[0],
        down_weight[0],
        out_weight,
        expert_tokens,
        norm_gain.reshape(1, width),
        expert_choice.T,
        route_weights.T,
    )


def solution(mesh):
    placed = (
        P("ep", "tp"),
        P("ep", "tp"),
        P("ep", "tp"),
        P("ep", "tp"),
        P("tp", None),
        P(("ep", "tp"), None),
        P(),
        P("ep", None, "tp"),
        P("ep", None, "tp"),
        P("ep", "tp", None),
        P(("ep", "tp"), None),
        P(("ep", "tp"), None),
    )
    return jax.shard_map(
        functools.partial(local, mesh.shape["ep"], mesh.shape["tp"]),
        mesh=mesh,
        in_specs=placed,
        out_specs=(P(("ep", "tp"), None), P(("ep", "tp"), None)),
        check_vma=False,
    )
```

```python
import functools
import math

import jax
import jax.numpy as jnp
from jax import lax
from jax.experimental import pallas as pl
from jax.experimental.pallas import tpu as pltpu
from jax.sharding import PartitionSpec as P

SLOT = 16
SIDE = 4
HEAD = 64
MESH = pl.DeviceIdType.MESH

eps_norm = 1e-05
clamp_limit = 7.0
sig_alpha = 1.702
floor_score = -1e30


def gate_row(tile):
    return jnp.concatenate([tile[r : r + 1, :] for r in range(tile.shape[0])], axis=1)


def activate(g, u):
    g = jnp.minimum(g, clamp_limit)
    u = jnp.clip(u, -clamp_limit, clamp_limit)
    return (g * jax.nn.sigmoid(sig_alpha * g) * (u + 1.0)).astype(jnp.bfloat16)


def attend_block(q_ref, cq_ref, kv_ref, ck_ref, m_ref, l_ref, acc_ref, diagonal):
    tile = q_ref.shape[0] // 2
    ck_all_row = gate_row(ck_ref[...])
    for i in range(2):
        rows = pl.ds(i * tile, tile)
        width = (i + 1) * tile if diagonal else kv_ref.shape[0]
        kv = kv_ref[:width, :]
        ck_row = ck_all_row[:, :width]
        s = lax.dot_general(
            q_ref[rows, :], kv, (((1,), (1,)), ((), ())), preferred_element_type=jnp.float32
        )
        s = s + (cq_ref[rows, :] - ck_row)
        if diagonal:
            q_pos = i * tile + lax.broadcasted_iota(jnp.int32, (tile, width), 0)
            k_pos = lax.broadcasted_iota(jnp.int32, (tile, width), 1)
            s = jnp.where(k_pos <= q_pos, s, floor_score)
        top = jnp.max(s, axis=1, keepdims=True)
        if diagonal:
            p = jnp.exp(s - top)
            m_ref[rows, :] = jnp.broadcast_to(top, (tile, 128))
            l_ref[rows, :] = jnp.broadcast_to(jnp.sum(p, axis=1, keepdims=True), (tile, 128))
            acc_ref[rows, :] = jnp.dot(
                p.astype(jnp.bfloat16), kv, preferred_element_type=jnp.float32
            )
        else:
            old = m_ref[rows, :]
            new = jnp.maximum(old, top)
            shrink = jnp.exp(old - new)
            p = jnp.exp(s - new[:, :1])
            m_ref[rows, :] = new
            l_ref[rows, :] = l_ref[rows, :] * shrink + jnp.sum(p, axis=1, keepdims=True)
            acc_ref[rows, :] = acc_ref[rows, :] * shrink + jnp.dot(
                p.astype(jnp.bfloat16), kv, preferred_element_type=jnp.float32
            )


SHARES = (5, 5, 4, 2)
N_BLOCKS = len(SHARES)
DOWN_ORDER = {
    3: ((0, 0), (1, 0), (2, 0), (0, 1), (1, 1), (0, 2), (2, 1), (0, 3), (1, 2), (3, 0),
        (1, 3), (2, 2), (3, 1), (2, 3), (3, 2), (3, 3)),
    1: ((0, 0), (1, 0), (2, 0), (0, 1), (1, 1), (3, 0), (2, 1), (3, 1)),
}


def body(
    n_ep,
    n_tp,
    qt_in,
    kt_in,
    vt_in,
    ck_ref,
    wg_in,
    wu_in,
    wd_in,
    ow_in,
    tok_in,
    gain_ref,
    choice_ref,
    route_ref,
    mix_ref,
    eo_ref,
    qt_ref,
    kt_ref,
    vt_ref,
    wg_ref,
    wu_ref,
    ow_ref,
    tok_ref,
    q_ref,
    cq_ref,
    og_ref,
    comb_ref,
    kv_all,
    ck_all,
    rg,
    ru,
    lg,
    lu,
    dn,
    act,
    x,
    acc,
    p_send,
    p_recv,
    res,
    ret,
    w_all,
    att_send,
    att_in,
    heads_ref,
    mix_acc,
    mp_send,
    mp_recv,
    m_ref,
    l_ref,
    att_acc,
    s_kv,
    r_kv,
    s_ck,
    r_ck,
    s_og,
    r_og,
    s_w,
    r_w,
    s_osl,
    r_osl,
    s_att,
    r_att,
    s_res,
    r_res,
    s_ring,
    r_ring,
    s_pt,
    r_pt,
    s_in,
):
    bf16, f32 = jnp.bfloat16, jnp.float32
    nz = n_tp // 2
    hops = nz // 2 - 1
    ep = lax.axis_index("ep")
    tp = lax.axis_index("tp")
    z = lax.div(tp, 2)
    core = lax.rem(tp, 2)
    right = lax.rem(tp + 2, n_tp)
    left = lax.rem(tp + n_tp - 2, n_tp)
    partner = tp + 1 - 2 * core
    units, width = wd_in.shape
    block = q_ref.shape[0]
    tokens = tok_ref.shape[0]
    slots_all = n_ep * SLOT
    col = width // n_ep
    unit = width // 16
    sizes = [n * unit for n in SHARES]
    offsets = [sum(sizes[:b]) for b in range(N_BLOCKS)]
    t_dev = mp_send.shape[0]

    def ep_peer(d):
        return lax.rem(ep + d, n_ep)

    def z_peer(d):
        return lax.rem(z + d, nz)

    def ep_copy(src, dst, send, recv, peer):
        return pltpu.make_async_remote_copy(
            src_ref=src, dst_ref=dst, send_sem=send, recv_sem=recv,
            device_id={"ep": peer}, device_id_type=MESH,
        )

    def tp_copy(src, dst, send, recv, peer):
        return pltpu.make_async_remote_copy(
            src_ref=src, dst_ref=dst, send_sem=send, recv_sem=recv,
            device_id={"tp": peer}, device_id_type=MESH,
        )

    y = lax.div(ep, SIDE)
    x_at = lax.rem(ep, SIDE)
    x_next = y * SIDE + lax.rem(x_at + 1, SIDE)
    x_prev = y * SIDE + lax.rem(x_at + SIDE - 1, SIDE)
    x_far = y * SIDE + lax.rem(x_at + 2, SIDE)
    y_next = lax.rem(y + 1, SIDE)
    y_prev = lax.rem(y + SIDE - 1, SIDE)
    y_far = lax.rem(y + 2, SIDE)

    class Spread:
        def __init__(self, buf, send, recv):
            self.buf, self.send, self.recv = buf, send, recv
            self.half = buf.shape[1] // 2

        def move(self, n, region, peer):
            return ep_copy(region, region, self.send.at[n], self.recv.at[n], peer)

        def part(self, slot, n):
            return self.buf.at[slot, pl.ds(n * self.half, self.half)]

        def rows(self, row, n, count):
            return self.buf.at[pl.ds(row * SIDE + n, count)]

        def sent(self, step):
            if step == 1:
                return (
                    self.move(0, self.buf.at[ep], x_next),
                    self.move(1, self.buf.at[ep], x_prev),
                )
            if step == 2:
                return (
                    self.move(2, self.part(x_prev, 0), x_next),
                    self.move(3, self.part(x_next, 1), x_prev),
                )
            up, down = y_next * SIDE + x_at, y_prev * SIDE + x_at
            if step == 3:
                return (
                    self.move(4, self.rows(y, 0, SIDE), up),
                    self.move(5, self.rows(y, 0, SIDE), down),
                )
            return (
                self.move(6, self.rows(y_prev, 0, SIDE // 2), up),
                self.move(7, self.rows(y_next, SIDE // 2, SIDE // 2), down),
            )

        def come(self, step):
            if step == 1:
                return (
                    self.move(0, self.buf.at[x_prev], x_next),
                    self.move(1, self.buf.at[x_next], x_prev),
                )
            if step == 2:
                return (
                    self.move(2, self.part(x_far, 0), x_next),
                    self.move(3, self.part(x_far, 1), x_prev),
                )
            up, down = y_next * SIDE + x_at, y_prev * SIDE + x_at
            if step == 3:
                return (
                    self.move(4, self.rows(y_prev, 0, SIDE), up),
                    self.move(5, self.rows(y_next, 0, SIDE), down),
                )
            return (
                self.move(6, self.rows(y_far, 0, SIDE // 2), up),
                self.move(7, self.rows(y_far, SIDE // 2, SIDE // 2), down),
            )

        def wait(self, step):
            for copy in self.come(step):
                copy.wait_recv()

        def start(self, step):
            for copy in self.sent(step):
                copy.start()

        def done(self):
            for step in range(1, 5):
                for copy in self.sent(step):
                    copy.wait_send()

    kv_spread = Spread(kv_all, s_kv, r_kv)
    w_spread = Spread(w_all, s_w, r_w)

    def ck_copy(slot, peer):
        return ep_copy(ck_ref, ck_all.at[slot], s_ck.at[peer], r_ck.at[slot], peer)

    def og_copy(slot, peer):
        return ep_copy(og_ref.at[peer], x.at[0, slot], s_og.at[peer], r_og.at[slot], peer)

    def res_copy(b, slot, peer):
        return ep_copy(
            res.at[b, peer, :, pl.ds(0, sizes[b])],
            ret.at[b, slot, :, pl.ds(0, sizes[b])],
            s_res.at[b, peer], r_res.at[b, slot], peer
        )

    my_cols = pl.ds(pl.multiple_of(ep * col, col), col)

    def osl_copy(slot, pz):
        return tp_copy(
            ow_ref.at[:, my_cols], w_all.at[ep, slot], s_osl.at[pz], r_osl.at[slot], 2 * pz + core
        )

    def att_copy(slot, pz):
        return tp_copy(
            att_send.at[pz], att_in.at[slot], s_att.at[pz], r_att.at[slot], 2 * pz + core
        )

    def pt_copy(src, dst, n):
        return tp_copy(src, dst, s_pt.at[n], r_pt.at[n], partner)

    def x_copy():
        return pt_copy(x.at[0], x.at[1], 0)

    def mp_copy():
        return pt_copy(mp_send, mp_recv, 1)

    def p_copy(b):
        cols = pl.ds(0, sizes[b])
        return pt_copy(p_send.at[b, :, cols], p_recv.at[b, :, cols], 2 + b)

    peers = (right, left)
    own = (wg_in, wu_in)
    slots = (rg, ru)
    last = (lg, lu)
    firsts = 2 * hops + 1
    down_order = DOWN_ORDER[hops]
    items = firsts + len(down_order)

    def gu_copy(direction, h, j):
        a = j if direction == 0 else 1 - j
        n = 2 * h + j
        sems = (s_ring.at[direction, n], r_ring.at[direction, n])
        return lambda src, dst: tp_copy(src, dst, *sems, peers[direction]), a

    def gu_first(direction, j):
        make, a = gu_copy(direction, 0, j)
        return make(own[a], slots[a].at[direction, 0])

    def gu_next(direction, h, j):
        make, a = gu_copy(direction, h, j)
        return make(slots[a].at[direction, h - 1], slots[a].at[direction, h])

    def gu_last(direction):
        make, a = gu_copy(direction, hops, 0)
        return make(slots[a].at[direction, hops - 1], last[a])

    def down_copy(direction, i):
        b, h = down_order[i]
        cols = pl.ds(offsets[b], sizes[b])
        n = firsts + i
        rows = pl.ds(0, units)
        to = 1 + 2 * h + direction
        if h == hops:
            rows = pl.ds(direction * (units // 2), units // 2)
            to = 1 + 2 * hops
        if h == 0:
            src = dn.at[0, rows, cols]
        else:
            src = dn.at[1 + 2 * (h - 1) + direction, rows, cols]
        return tp_copy(
            src, dn.at[to, rows, cols], s_ring.at[direction, n], r_ring.at[direction, n],
            peers[direction],
        )

    def start_down(i):
        for direction in range(2):
            down_copy(direction, i).start()

    def each(start, stop, fn):
        def run(d, carry):
            fn(d)
            return carry

        lax.fori_loop(start, stop, run, 0)

    loads = [
        pltpu.make_async_copy(src, dst, s_in.at[n])
        for n, (src, dst) in enumerate(
            (
                (ow_in, ow_ref),
                (kt_in, kt_ref),
                (vt_in, vt_ref),
                (qt_in, qt_ref),
                (tok_in, tok_ref),
                (wg_in, wg_ref),
                (wu_in, wu_ref),
                (wd_in, dn.at[0]),
            )
        )
    ]
    for load in loads:
        load.start()

    barrier = pltpu.get_barrier_semaphore()
    each(
        1, n_ep,
        lambda d: pl.semaphore_signal(
            barrier, inc=1, device_id={"ep": ep_peer(d)}, device_id_type=MESH
        ),
    )
    each(
        1, nz,
        lambda d: pl.semaphore_signal(
            barrier, inc=1, device_id={"tp": 2 * z_peer(d) + core}, device_id_type=MESH
        ),
    )
    pl.semaphore_signal(barrier, inc=1, device_id={"tp": partner}, device_id_type=MESH)
    pl.semaphore_wait(barrier, n_ep - 1 + nz - 1 + 1)

    for direction in range(2):
        gu_first(direction, 0).start()
    loads[0].wait()
    each(1, nz, lambda d: osl_copy(z, z_peer(d)).start())
    for direction in range(2):
        gu_first(direction, 1).start()
    for load in loads[1:]:
        load.wait()

    kv_all[ep] = (
        jnp.concatenate([kt_ref[...].astype(f32), vt_ref[...].astype(f32)], axis=0)
        .T.astype(bf16)
    )
    scaled = qt_ref[...].astype(f32) * (1.0 / math.sqrt(HEAD))
    q_ref[...] = jnp.concatenate([scaled, jnp.zeros_like(scaled)], axis=0).T.astype(bf16)
    turned = ck_ref[...].T
    for r in range(block // 128):
        cq_ref[pl.ds(r * 128, 128), :] = turned[:, r : r + 1]

    ids = choice_ref[...]
    e_pos = lax.broadcasted_iota(jnp.int32, (n_ep, tokens), 0)
    named = [(e_pos == ids[k : k + 1, :]).astype(f32) for k in range(ids.shape[0])]
    both = functools.reduce(jnp.add, named)
    before = (
        lax.broadcasted_iota(jnp.int32, (tokens, tokens), 0)
        < lax.broadcasted_iota(jnp.int32, (tokens, tokens), 1)
    )
    earlier = jnp.dot(
        both.astype(bf16), before.astype(f32).astype(bf16), preferred_element_type=f32
    )
    s_pos = lax.broadcasted_iota(jnp.int32, (slots_all, tokens), 0).astype(f32)
    placing = jnp.zeros((slots_all, tokens), f32)
    comb = jnp.zeros((slots_all, tokens), f32)
    for k in range(ids.shape[0]):
        rank = jnp.sum(named[k] * earlier, axis=0, keepdims=True)
        slot = ids[k : k + 1, :].astype(f32) * SLOT + rank
        here = s_pos == slot
        placing = jnp.where(here, 1.0, placing)
        comb = jnp.where(here, route_ref[k : k + 1, :], comb)
    comb_ref[...] = comb.T
    tok = tok_ref[...].astype(f32)
    normed = (
        tok * lax.rsqrt(jnp.mean(tok * tok, axis=1, keepdims=True) + eps_norm) * gain_ref[...]
    ).astype(bf16)
    og_ref[...] = (
        jnp.dot(placing.astype(bf16), normed, preferred_element_type=f32)
        .astype(bf16)
        .reshape(n_ep, SLOT, width)
    )

    attend_block(q_ref, cq_ref, kv_all.at[ep], ck_ref, m_ref, l_ref, att_acc, True)

    kv_spread.start(1)
    each(1, n_ep - ep, lambda d: ck_copy(ep, ep + d).start())
    each(1, n_ep, lambda d: og_copy(ep, ep_peer(d)).start())
    x[0, ep] = og_ref[ep]
    w_all[ep, z] = ow_ref[:, my_cols]

    def attend_step(j):
        ck_copy(j, j).wait_recv()
        attend_block(q_ref, cq_ref, kv_all.at[j], ck_all.at[j], m_ref, l_ref, att_acc, False)

    def expert_units(g_ref, u_ref, n):
        cols = pl.ds(pl.multiple_of(n * units, units), units)
        for half in range(2):
            rows = x[half].reshape(slots_all, width)
            g = jnp.dot(rows, g_ref[...], preferred_element_type=f32)
            u = jnp.dot(rows, u_ref[...], preferred_element_type=f32)
            act[half, :, cols] = activate(g, u)

    def units_of(h):
        for direction in range(2):
            expert_units(rg.at[direction, h], ru.at[direction, h], 1 + 2 * h + direction)

    def kv_step(step):
        kv_spread.wait(step - 1)
        kv_spread.start(step)

    def w_step(step):
        w_spread.wait(step - 1)
        w_spread.start(step)

    def first_w():
        each(1, nz, lambda d: osl_copy(z_peer(d), z_peer(d)).wait_recv())
        w_spread.start(1)

    def swap_rows():
        each(1, n_ep, lambda d: og_copy(ep_peer(d), ep_peer(d)).wait_recv())
        x_copy().start()

    def own_units():
        x_copy().wait_recv()
        expert_units(wg_ref, wu_ref, 0)

    def send_attention():
        for pz in range(nz):
            rows = pl.ds(pz * 2 * t_dev, 2 * t_dev)
            o = (att_acc[rows, :] / l_ref[rows, :])[:, HEAD:]
            att_send[pz] = jnp.concatenate([o[:t_dev], o[t_dev:]], axis=1).astype(bf16)
        att_in[z] = att_send[z]

    def above(n):
        return SIDE * jnp.maximum(y - n, 0)

    def units_safe(h):
        if h < hops:
            units_of(h)

    work_list = [
        (0, lambda: kv_step(2)),
        (0, first_w),
        (1, lambda: kv_step(3)),
        (1, swap_rows),
        (1, lambda: each(SIDE * y, ep, attend_step)),
        (1, lambda: w_step(2)),
        (2, own_units),
        (2, lambda: units_safe(0)),
        (3, lambda: kv_step(4)),
        (3, lambda: each(above(1), SIDE * y, attend_step)),
        (4, lambda: w_step(3)),
        (4, lambda: units_safe(1)),
        (4, lambda: each(0, above(2), attend_step)),
        (5, lambda: kv_spread.wait(4)),
        (5, lambda: each(above(2), above(1), attend_step)),
        (6, send_attention),
        (6, lambda: w_step(4)),
        (6, lambda: units_safe(2)),
    ]
    for n in range(firsts):
        h, j = n // 2, n % 2
        for direction in range(2):
            if n == firsts - 1:
                gu_last(direction).wait_recv()
            elif h == 0:
                gu_first(direction, j).wait_recv()
            else:
                gu_next(direction, h, j).wait_recv()
            follow = n + 2
            if follow < firsts - 1:
                gu_next(direction, h + 1, j).start()
            elif follow == firsts - 1:
                gu_last(direction).start()
        if n == firsts - 2:
            for i in range(3):
                start_down(i)
        for at, work in work_list:
            if min(at, firsts - 1) == n:
                work()
    each(1, nz, lambda d: att_copy(z, z_peer(d)).start())
    expert_units(lg, lu, 1 + 2 * hops)

    def gather_heads():
        each(1, nz, lambda d: att_copy(z_peer(d), z_peer(d)).wait_recv())
        got = [att_in[pz].astype(f32) for pz in range(nz)]
        heads_ref[pl.ds(0, t_dev), :] = jnp.concatenate(
            [t[:, :HEAD] for t in got], axis=1
        ).astype(bf16)
        heads_ref[pl.ds(t_dev, t_dev), :] = jnp.concatenate(
            [t[:, HEAD:] for t in got], axis=1
        ).astype(bf16)
        w_spread.wait(4)

    def project(e):
        piece = w_all[e].reshape(nz * HEAD, col)
        mix_acc[:, pl.ds(pl.multiple_of(e * col, col), col)] = jnp.dot(
            heads_ref[...], piece, preferred_element_type=f32
        )

    theirs = pl.ds(pl.multiple_of((1 - core) * t_dev, t_dev), t_dev)
    mine = pl.ds(pl.multiple_of(core * t_dev, t_dev), t_dev)

    def send_mix():
        mp_send[...] = mix_acc[theirs, :].astype(bf16)
        mp_copy().start()

    def take_mix():
        mp_copy().wait_recv()
        mix_ref[...] = (mix_acc[mine, :] + mp_recv[...].astype(f32)).astype(bf16)

    def finish_units(b):
        size = sizes[b]
        weights = dn[:, :, offsets[b] : offsets[b] + size].reshape(nz * units, size)
        p_send[b, :, :size] = jnp.dot(act[1], weights, preferred_element_type=f32).astype(bf16)
        p_copy(b).start()
        acc[b, :, :size] = jnp.dot(act[0], weights, preferred_element_type=f32)

    def send_home(b):
        p_copy(b).wait_recv()
        size = sizes[b]
        total = acc[b, :, :size] + p_recv[b, :, :size].astype(f32)
        res[b, :, :, :size] = total.astype(bf16).reshape(n_ep, SLOT, size)
        each(1, n_ep, lambda d: res_copy(b, ep, ep_peer(d)).start())
        ret[b, ep, :, :size] = res[b, ep, :, :size]

    c0 = comb_ref[...]
    c_hi = c0.astype(bf16)
    c1 = c0 - c_hi.astype(f32)
    c_mid = c1.astype(bf16)
    c_lo = (c1 - c_mid.astype(f32)).astype(bf16)

    def combine(b):
        each(1, n_ep, lambda d: res_copy(b, ep_peer(d), ep_peer(d)).wait_recv())
        size = sizes[b]
        back = ret[b, :, :, :size].reshape(slots_all, size)
        total = jnp.dot(c_hi, back, preferred_element_type=f32)
        total += jnp.dot(c_mid, back, preferred_element_type=f32)
        total += jnp.dot(c_lo, back, preferred_element_type=f32)
        eo_ref[:, offsets[b] : offsets[b] + size] = total.astype(bf16)

    count = len(down_order)
    issued = 3
    arrived = []
    pending = []
    mixer_work = [gather_heads]
    quarter = -(-n_ep // 4)
    for q in range(4):
        mixer_work.append(
            functools.partial(each, q * quarter, min((q + 1) * quarter, n_ep), project)
        )
    mixer_work += [send_mix, take_mix]
    mixer_at = min(4, count - 8) if count > 8 else 0
    for i in range(count):
        for direction in range(2):
            down_copy(direction, i).wait_recv()
        arrived.append(down_order[i])
        while issued < min(count, i + 3):
            b, h = down_order[issued]
            if h > 0 and (b, h - 1) not in arrived:
                break
            start_down(issued)
            issued += 1
        for b in pending:
            send_home(b)
        pending = []
        b, h = down_order[i]
        if h == hops:
            finish_units(b)
            pending.append(b)
        elif i >= mixer_at and mixer_work:
            mixer_work.pop(0)()
    for b in pending:
        send_home(b)
    for work in mixer_work:
        work()

    each(1, nz, lambda d: osl_copy(z, z_peer(d)).wait_send())
    each(1, nz, lambda d: att_copy(z, z_peer(d)).wait_send())
    for direction in range(2):
        for j in range(2):
            gu_first(direction, j).wait_send()
            each(1, hops, lambda h: gu_next(direction, h, j).wait_send())
        gu_last(direction).wait_send()
        for i in range(count):
            down_copy(direction, i).wait_send()
    each(1, n_ep, lambda d: og_copy(ep, ep_peer(d)).wait_send())
    kv_spread.done()
    w_spread.done()
    each(1, n_ep - ep, lambda d: ck_copy(ep, ep + d).wait_send())
    x_copy().wait_send()
    mp_copy().wait_send()
    for b in range(N_BLOCKS):
        p_copy(b).wait_send()
    for b in range(N_BLOCKS):
        combine(b)
    for b in range(N_BLOCKS):
        each(1, n_ep, lambda d: res_copy(b, ep, ep_peer(d)).wait_send())


def local(
    n_ep,
    n_tp,
    queries,
    key_vectors,
    value_vectors,
    cumulative_gate,
    out_weight,
    expert_tokens,
    norm_gain,
    gate_weight,
    up_weight,
    down_weight,
    expert_choice,
    route_weights,
):
    tokens, width = expert_tokens.shape
    block, head = queries.shape
    units = gate_weight.shape[2]
    nz = n_tp // 2
    hops = nz // 2 - 1
    t_dev = block // n_tp
    col = width // n_ep
    part = max(SHARES) * width // 16
    slots_all = n_ep * SLOT
    items = 2 * hops + 1 + len(DOWN_ORDER[hops])
    bf16, f32 = jnp.bfloat16, jnp.float32
    dma = pltpu.SemaphoreType.DMA
    vmem = pltpu.VMEM
    return pl.pallas_call(
        functools.partial(body, n_ep, n_tp),
        out_shape=(
            jax.ShapeDtypeStruct((t_dev, width), bf16),
            jax.ShapeDtypeStruct((tokens, width), bf16),
        ),
        in_specs=[
            pl.BlockSpec(memory_space=vmem if n in (3, 9, 10, 11) else pl.ANY) for n in range(12)
        ],
        out_specs=(pl.BlockSpec(memory_space=vmem),) * 2,
        scratch_shapes=[
            vmem((head, block), bf16),
            vmem((head, block), bf16),
            vmem((head, block), bf16),
            vmem((width, units), bf16),
            vmem((width, units), bf16),
            vmem((head, width), bf16),
            vmem((tokens, width), bf16),
            vmem((block, 128), bf16),
            vmem((block, 1), f32),
            vmem((n_ep, SLOT, width), bf16),
            vmem((tokens, slots_all), f32),
            vmem((n_ep, block, 128), bf16),
            vmem((n_ep, block // 128, 128), f32),
            vmem((2, hops, width, units), bf16),
            vmem((2, hops, width, units), bf16),
            vmem((width, units), bf16),
            vmem((width, units), bf16),
            vmem((nz, units, width), bf16),
            vmem((2, slots_all, nz * units), bf16),
            vmem((2, n_ep, SLOT, width), bf16),
            vmem((N_BLOCKS, slots_all, part), f32),
            vmem((N_BLOCKS, slots_all, part), bf16),
            vmem((N_BLOCKS, slots_all, part), bf16),
            vmem((N_BLOCKS, n_ep, SLOT, part), bf16),
            vmem((N_BLOCKS, n_ep, SLOT, part), bf16),
            vmem((n_ep, nz, head, col), bf16),
            vmem((nz, t_dev, 128), bf16),
            vmem((nz, t_dev, 128), bf16),
            vmem((2 * t_dev, nz * head), bf16),
            vmem((2 * t_dev, width), f32),
            vmem((t_dev, width), bf16),
            vmem((t_dev, width), bf16),
            vmem((block, 128), f32),
            vmem((block, 128), f32),
            vmem((block, 128), f32),
        ]
        + [dma((8,))] * 2
        + [dma((n_ep,))] * 4
        + [dma((8,))] * 2
        + [dma((nz,))] * 4
        + [dma((N_BLOCKS, n_ep))] * 2
        + [dma((2, items))] * 2
        + [dma((2 + N_BLOCKS,))] * 2
        + [dma((8,))],
        compiler_params=pltpu.CompilerParams(
            collective_id=0, has_side_effects=True, vmem_limit_bytes=63 * 2**20
        ),
        name="whole",
    )(
        queries.T,
        key_vectors.T,
        value_vectors.T,
        cumulative_gate.reshape(block // 128, 128),
        gate_weight[0],
        up_weight[0],
        down_weight[0],
        out_weight,
        expert_tokens,
        norm_gain.reshape(1, width),
        expert_choice.T,
        route_weights.T,
    )


def solution(mesh):
    placed = (
        P("ep", "tp"),
        P("ep", "tp"),
        P("ep", "tp"),
        P("ep", "tp"),
        P("tp", None),
        P(("ep", "tp"), None),
        P(),
        P("ep", None, "tp"),
        P("ep", None, "tp"),
        P("ep", "tp", None),
        P(("ep", "tp"), None),
        P(("ep", "tp"), None),
    )
    return jax.shard_map(
        functools.partial(local, mesh.shape["ep"], mesh.shape["tp"]),
        mesh=mesh,
        in_specs=placed,
        out_specs=(P(("ep", "tp"), None), P(("ep", "tp"), None)),
        check_vma=False,
    )
```

```python
import functools
import math

import jax
import jax.numpy as jnp
from jax import lax
from jax.experimental import pallas as pl
from jax.experimental.pallas import tpu as pltpu
from jax.sharding import PartitionSpec as P

SLOT = 16
SIDE = 4
HEAD = 64
MESH = pl.DeviceIdType.MESH

eps_norm = 1e-05
clamp_limit = 7.0
sig_alpha = 1.702
floor_score = -1e30


def gate_row(tile):
    return jnp.concatenate([tile[r : r + 1, :] for r in range(tile.shape[0])], axis=1)


def activate(g, u):
    g = jnp.minimum(g, clamp_limit)
    u = jnp.clip(u, -clamp_limit, clamp_limit)
    return (g * jax.nn.sigmoid(sig_alpha * g) * (u + 1.0)).astype(jnp.bfloat16)


def attend_block(q_ref, cq_ref, kv_ref, ck_ref, m_ref, l_ref, acc_ref, diagonal):
    tile = q_ref.shape[0] // 2
    ck_all_row = gate_row(ck_ref[...])
    for i in range(2):
        rows = pl.ds(i * tile, tile)
        width = (i + 1) * tile if diagonal else kv_ref.shape[0]
        kv = kv_ref[:width, :]
        ck_row = ck_all_row[:, :width]
        s = lax.dot_general(
            q_ref[rows, :], kv, (((1,), (1,)), ((), ())), preferred_element_type=jnp.float32
        )
        s = s + (cq_ref[rows, :] - ck_row)
        if diagonal:
            q_pos = i * tile + lax.broadcasted_iota(jnp.int32, (tile, width), 0)
            k_pos = lax.broadcasted_iota(jnp.int32, (tile, width), 1)
            s = jnp.where(k_pos <= q_pos, s, floor_score)
        top = jnp.max(s, axis=1, keepdims=True)
        if diagonal:
            p = jnp.exp(s - top)
            m_ref[rows, :] = jnp.broadcast_to(top, (tile, 128))
            l_ref[rows, :] = jnp.broadcast_to(jnp.sum(p, axis=1, keepdims=True), (tile, 128))
            acc_ref[rows, :] = jnp.dot(
                p.astype(jnp.bfloat16), kv, preferred_element_type=jnp.float32
            )
        else:
            old = m_ref[rows, :]
            new = jnp.maximum(old, top)
            shrink = jnp.exp(old - new)
            p = jnp.exp(s - new[:, :1])
            m_ref[rows, :] = new
            l_ref[rows, :] = l_ref[rows, :] * shrink + jnp.sum(p, axis=1, keepdims=True)
            acc_ref[rows, :] = acc_ref[rows, :] * shrink + jnp.dot(
                p.astype(jnp.bfloat16), kv, preferred_element_type=jnp.float32
            )


SHARES = (5, 5, 4, 2)
N_BLOCKS = len(SHARES)
DOWN_ORDER = {
    3: ((0, 0), (1, 0), (2, 0), (1, 1), (0, 1), (1, 2), (0, 2), (1, 3), (2, 1), (0, 3),
        (3, 0), (2, 2), (3, 1), (2, 3), (3, 2), (3, 3)),
    1: ((0, 0), (1, 0), (2, 0), (0, 1), (1, 1), (3, 0), (2, 1), (3, 1)),
}


def body(
    n_ep,
    n_tp,
    qt_in,
    kt_in,
    vt_in,
    ck_ref,
    wg_in,
    wu_in,
    wd_in,
    ow_in,
    tok_in,
    gain_ref,
    choice_ref,
    route_ref,
    mix_ref,
    eo_ref,
    qt_ref,
    kt_ref,
    vt_ref,
    wg_ref,
    wu_ref,
    ow_ref,
    tok_ref,
    q_ref,
    cq_ref,
    og_ref,
    comb_ref,
    kv_all,
    ck_all,
    rg,
    ru,
    lg,
    lu,
    dn,
    act,
    x,
    acc,
    p_send,
    p_recv,
    res,
    ret,
    w_all,
    att_send,
    att_in,
    heads_ref,
    mix_acc,
    mp_send,
    mp_recv,
    m_ref,
    l_ref,
    att_acc,
    s_kv,
    r_kv,
    s_ck,
    r_ck,
    s_og,
    r_og,
    s_w,
    r_w,
    s_osl,
    r_osl,
    s_att,
    r_att,
    s_res,
    r_res,
    s_ring,
    r_ring,
    s_pt,
    r_pt,
    s_in,
):
    bf16, f32 = jnp.bfloat16, jnp.float32
    nz = n_tp // 2
    hops = nz // 2 - 1
    ep = lax.axis_index("ep")
    tp = lax.axis_index("tp")
    z = lax.div(tp, 2)
    core = lax.rem(tp, 2)
    right = lax.rem(tp + 2, n_tp)
    left = lax.rem(tp + n_tp - 2, n_tp)
    partner = tp + 1 - 2 * core
    units, width = wd_in.shape
    block = q_ref.shape[0]
    tokens = tok_ref.shape[0]
    slots_all = n_ep * SLOT
    col = width // n_ep
    unit = width // 16
    sizes = [n * unit for n in SHARES]
    offsets = [sum(sizes[:b]) for b in range(N_BLOCKS)]
    t_dev = mp_send.shape[0]

    def ep_peer(d):
        return lax.rem(ep + d, n_ep)

    def z_peer(d):
        return lax.rem(z + d, nz)

    def ep_copy(src, dst, send, recv, peer):
        return pltpu.make_async_remote_copy(
            src_ref=src, dst_ref=dst, send_sem=send, recv_sem=recv,
            device_id={"ep": peer}, device_id_type=MESH,
        )

    def tp_copy(src, dst, send, recv, peer):
        return pltpu.make_async_remote_copy(
            src_ref=src, dst_ref=dst, send_sem=send, recv_sem=recv,
            device_id={"tp": peer}, device_id_type=MESH,
        )

    y = lax.div(ep, SIDE)
    x_at = lax.rem(ep, SIDE)
    x_next = y * SIDE + lax.rem(x_at + 1, SIDE)
    x_prev = y * SIDE + lax.rem(x_at + SIDE - 1, SIDE)
    x_far = y * SIDE + lax.rem(x_at + 2, SIDE)
    y_next = lax.rem(y + 1, SIDE)
    y_prev = lax.rem(y + SIDE - 1, SIDE)
    y_far = lax.rem(y + 2, SIDE)

    class Spread:
        def __init__(self, buf, send, recv):
            self.buf, self.send, self.recv = buf, send, recv
            self.half = buf.shape[1] // 2

        def move(self, n, region, peer):
            return ep_copy(region, region, self.send.at[n], self.recv.at[n], peer)

        def part(self, slot, n):
            return self.buf.at[slot, pl.ds(n * self.half, self.half)]

        def rows(self, row, n, count):
            return self.buf.at[pl.ds(row * SIDE + n, count)]

        def sent(self, step):
            if step == 1:
                return (
                    self.move(0, self.buf.at[ep], x_next),
                    self.move(1, self.buf.at[ep], x_prev),
                )
            if step == 2:
                return (
                    self.move(2, self.part(x_prev, 0), x_next),
                    self.move(3, self.part(x_next, 1), x_prev),
                )
            up, down = y_next * SIDE + x_at, y_prev * SIDE + x_at
            if step == 3:
                return (
                    self.move(4, self.rows(y, 0, SIDE), up),
                    self.move(5, self.rows(y, 0, SIDE), down),
                )
            return (
                self.move(6, self.rows(y_prev, 0, SIDE // 2), up),
                self.move(7, self.rows(y_next, SIDE // 2, SIDE // 2), down),
            )

        def come(self, step):
            if step == 1:
                return (
                    self.move(0, self.buf.at[x_prev], x_next),
                    self.move(1, self.buf.at[x_next], x_prev),
                )
            if step == 2:
                return (
                    self.move(2, self.part(x_far, 0), x_next),
                    self.move(3, self.part(x_far, 1), x_prev),
                )
            up, down = y_next * SIDE + x_at, y_prev * SIDE + x_at
            if step == 3:
                return (
                    self.move(4, self.rows(y_prev, 0, SIDE), up),
                    self.move(5, self.rows(y_next, 0, SIDE), down),
                )
            return (
                self.move(6, self.rows(y_far, 0, SIDE // 2), up),
                self.move(7, self.rows(y_far, SIDE // 2, SIDE // 2), down),
            )

        def wait(self, step):
            for copy in self.come(step):
                copy.wait_recv()

        def start(self, step):
            for copy in self.sent(step):
                copy.start()

        def done(self):
            for step in range(1, 5):
                for copy in self.sent(step):
                    copy.wait_send()

    kv_spread = Spread(kv_all, s_kv, r_kv)
    w_spread = Spread(w_all, s_w, r_w)

    def ck_copy(slot, peer):
        return ep_copy(ck_ref, ck_all.at[slot], s_ck.at[peer], r_ck.at[slot], peer)

    def og_copy(slot, peer):
        return ep_copy(og_ref.at[peer], x.at[0, slot], s_og.at[peer], r_og.at[slot], peer)

    def res_copy(b, slot, peer):
        return ep_copy(
            res.at[b, peer, :, pl.ds(0, sizes[b])],
            ret.at[b, slot, :, pl.ds(0, sizes[b])],
            s_res.at[b, peer], r_res.at[b, slot], peer
        )

    my_cols = pl.ds(pl.multiple_of(ep * col, col), col)

    def osl_copy(slot, pz):
        return tp_copy(
            ow_ref.at[:, my_cols], w_all.at[ep, slot], s_osl.at[pz], r_osl.at[slot], 2 * pz + core
        )

    def att_copy(slot, pz):
        return tp_copy(
            att_send.at[pz], att_in.at[slot], s_att.at[pz], r_att.at[slot], 2 * pz + core
        )

    def pt_copy(src, dst, n):
        return tp_copy(src, dst, s_pt.at[n], r_pt.at[n], partner)

    def x_copy():
        return pt_copy(x.at[0], x.at[1], 0)

    def mp_copy():
        return pt_copy(mp_send, mp_recv, 1)

    def p_copy(b):
        cols = pl.ds(0, sizes[b])
        return pt_copy(p_send.at[b, :, cols], p_recv.at[b, :, cols], 2 + b)

    peers = (right, left)
    own = (wg_ref, wu_ref)
    slots = (rg, ru)
    last = (lg, lu)
    firsts = 2 * hops + 1
    down_order = DOWN_ORDER[hops]
    items = firsts + len(down_order)

    def gu_copy(direction, h, j):
        a = j if direction == 0 else 1 - j
        n = 2 * h + j
        sems = (s_ring.at[direction, n], r_ring.at[direction, n])
        return lambda src, dst: tp_copy(src, dst, *sems, peers[direction]), a

    def gu_first(direction, j):
        make, a = gu_copy(direction, 0, j)
        return make(own[a], slots[a].at[direction, 0])

    def gu_next(direction, h, j):
        make, a = gu_copy(direction, h, j)
        return make(slots[a].at[direction, h - 1], slots[a].at[direction, h])

    def gu_last(direction):
        make, a = gu_copy(direction, hops, 0)
        return make(slots[a].at[direction, hops - 1], last[a])

    def down_copy(direction, i):
        b, h = down_order[i]
        cols = pl.ds(offsets[b], sizes[b])
        n = firsts + i
        rows = pl.ds(0, units)
        to = 1 + 2 * h + direction
        if h == hops:
            rows = pl.ds(direction * (units // 2), units // 2)
            to = 1 + 2 * hops
        if h == 0:
            src = dn.at[0, rows, cols]
        else:
            src = dn.at[1 + 2 * (h - 1) + direction, rows, cols]
        return tp_copy(
            src, dn.at[to, rows, cols], s_ring.at[direction, n], r_ring.at[direction, n],
            peers[direction],
        )

    def start_down(i):
        for direction in range(2):
            down_copy(direction, i).start()

    def each(start, stop, fn):
        def run(d, carry):
            fn(d)
            return carry

        lax.fori_loop(start, stop, run, 0)

    loads = [
        pltpu.make_async_copy(src, dst, s_in.at[n])
        for n, (src, dst) in enumerate(
            (
                (wg_in, wg_ref),
                (wu_in, wu_ref),
                (ow_in, ow_ref),
                (kt_in, kt_ref),
                (vt_in, vt_ref),
                (qt_in, qt_ref),
                (tok_in, tok_ref),
                (wd_in, dn.at[0]),
            )
        )
    ]
    for load in loads:
        load.start()

    barrier = pltpu.get_barrier_semaphore()
    each(
        1, n_ep,
        lambda d: pl.semaphore_signal(
            barrier, inc=1, device_id={"ep": ep_peer(d)}, device_id_type=MESH
        ),
    )
    each(
        1, nz,
        lambda d: pl.semaphore_signal(
            barrier, inc=1, device_id={"tp": 2 * z_peer(d) + core}, device_id_type=MESH
        ),
    )
    pl.semaphore_signal(barrier, inc=1, device_id={"tp": partner}, device_id_type=MESH)
    pl.semaphore_wait(barrier, n_ep - 1 + nz - 1 + 1)

    for load in loads[:3]:
        load.wait()
    for direction in range(2):
        gu_first(direction, 0).start()
    each(1, nz, lambda d: osl_copy(z, z_peer(d)).start())
    for direction in range(2):
        gu_first(direction, 1).start()
    for load in loads[3:]:
        load.wait()

    kv_all[ep] = (
        jnp.concatenate([kt_ref[...].astype(f32), vt_ref[...].astype(f32)], axis=0)
        .T.astype(bf16)
    )
    scaled = qt_ref[...].astype(f32) * (1.0 / math.sqrt(HEAD))
    q_ref[...] = jnp.concatenate([scaled, jnp.zeros_like(scaled)], axis=0).T.astype(bf16)
    turned = ck_ref[...].T
    for r in range(block // 128):
        cq_ref[pl.ds(r * 128, 128), :] = turned[:, r : r + 1]

    ids = choice_ref[...]
    e_pos = lax.broadcasted_iota(jnp.int32, (n_ep, tokens), 0)
    named = [(e_pos == ids[k : k + 1, :]).astype(f32) for k in range(ids.shape[0])]
    both = functools.reduce(jnp.add, named)
    before = (
        lax.broadcasted_iota(jnp.int32, (tokens, tokens), 0)
        < lax.broadcasted_iota(jnp.int32, (tokens, tokens), 1)
    )
    earlier = jnp.dot(
        both.astype(bf16), before.astype(f32).astype(bf16), preferred_element_type=f32
    )
    s_pos = lax.broadcasted_iota(jnp.int32, (slots_all, tokens), 0).astype(f32)
    placing = jnp.zeros((slots_all, tokens), f32)
    comb = jnp.zeros((slots_all, tokens), f32)
    for k in range(ids.shape[0]):
        rank = jnp.sum(named[k] * earlier, axis=0, keepdims=True)
        slot = ids[k : k + 1, :].astype(f32) * SLOT + rank
        here = s_pos == slot
        placing = jnp.where(here, 1.0, placing)
        comb = jnp.where(here, route_ref[k : k + 1, :], comb)
    comb_ref[...] = comb.T
    tok = tok_ref[...].astype(f32)
    normed = (
        tok * lax.rsqrt(jnp.mean(tok * tok, axis=1, keepdims=True) + eps_norm) * gain_ref[...]
    ).astype(bf16)
    og_ref[...] = (
        jnp.dot(placing.astype(bf16), normed, preferred_element_type=f32)
        .astype(bf16)
        .reshape(n_ep, SLOT, width)
    )

    attend_block(q_ref, cq_ref, kv_all.at[ep], ck_ref, m_ref, l_ref, att_acc, True)

    kv_spread.start(1)
    each(1, n_ep - ep, lambda d: ck_copy(ep, ep + d).start())
    each(1, n_ep, lambda d: og_copy(ep, ep_peer(d)).start())
    x[0, ep] = og_ref[ep]
    w_all[ep, z] = ow_ref[:, my_cols]

    def attend_step(j):
        ck_copy(j, j).wait_recv()
        attend_block(q_ref, cq_ref, kv_all.at[j], ck_all.at[j], m_ref, l_ref, att_acc, False)

    def expert_units(g_ref, u_ref, n):
        cols = pl.ds(pl.multiple_of(n * units, units), units)
        for half in range(2):
            rows = x[half].reshape(slots_all, width)
            g = jnp.dot(rows, g_ref[...], preferred_element_type=f32)
            u = jnp.dot(rows, u_ref[...], preferred_element_type=f32)
            act[half, :, cols] = activate(g, u)

    def units_of(h):
        for direction in range(2):
            expert_units(rg.at[direction, h], ru.at[direction, h], 1 + 2 * h + direction)

    def kv_step(step):
        kv_spread.wait(step - 1)
        kv_spread.start(step)

    def w_step(step):
        w_spread.wait(step - 1)
        w_spread.start(step)

    def first_w():
        each(1, nz, lambda d: osl_copy(z_peer(d), z_peer(d)).wait_recv())
        w_spread.start(1)

    def swap_rows():
        each(1, n_ep, lambda d: og_copy(ep_peer(d), ep_peer(d)).wait_recv())
        x_copy().start()

    def own_units():
        x_copy().wait_recv()
        expert_units(wg_ref, wu_ref, 0)

    def send_attention():
        for pz in range(nz):
            rows = pl.ds(pz * 2 * t_dev, 2 * t_dev)
            o = (att_acc[rows, :] / l_ref[rows, :])[:, HEAD:]
            att_send[pz] = jnp.concatenate([o[:t_dev], o[t_dev:]], axis=1).astype(bf16)
        att_in[z] = att_send[z]

    def above(n):
        return SIDE * jnp.maximum(y - n, 0)

    def units_safe(h):
        if h < hops:
            units_of(h)

    work_list = [
        (0, lambda: kv_step(2)),
        (0, first_w),
        (1, lambda: kv_step(3)),
        (1, swap_rows),
        (1, lambda: each(SIDE * y, ep, attend_step)),
        (1, lambda: w_step(2)),
        (2, own_units),
        (2, lambda: units_safe(0)),
        (3, lambda: kv_step(4)),
        (3, lambda: each(above(1), SIDE * y, attend_step)),
        (4, lambda: w_step(3)),
        (4, lambda: units_safe(1)),
        (4, lambda: each(0, above(2), attend_step)),
        (5, lambda: kv_spread.wait(4)),
        (5, lambda: each(above(2), above(1), attend_step)),
        (6, send_attention),
        (6, lambda: w_step(4)),
        (6, lambda: units_safe(2)),
    ]
    for n in range(firsts):
        h, j = n // 2, n % 2
        for direction in range(2):
            if n == firsts - 1:
                gu_last(direction).wait_recv()
            elif h == 0:
                gu_first(direction, j).wait_recv()
            else:
                gu_next(direction, h, j).wait_recv()
            follow = n + 2
            if follow < firsts - 1:
                gu_next(direction, h + 1, j).start()
            elif follow == firsts - 1:
                gu_last(direction).start()
        if n == firsts - 2:
            for i in range(3):
                start_down(i)
        for at, work in work_list:
            if min(at, firsts - 1) == n:
                work()
    each(1, nz, lambda d: att_copy(z, z_peer(d)).start())
    expert_units(lg, lu, 1 + 2 * hops)

    def gather_heads():
        each(1, nz, lambda d: att_copy(z_peer(d), z_peer(d)).wait_recv())
        got = [att_in[pz].astype(f32) for pz in range(nz)]
        heads_ref[pl.ds(0, t_dev), :] = jnp.concatenate(
            [t[:, :HEAD] for t in got], axis=1
        ).astype(bf16)
        heads_ref[pl.ds(t_dev, t_dev), :] = jnp.concatenate(
            [t[:, HEAD:] for t in got], axis=1
        ).astype(bf16)
        w_spread.wait(4)

    def project(e):
        piece = w_all[e].reshape(nz * HEAD, col)
        mix_acc[:, pl.ds(pl.multiple_of(e * col, col), col)] = jnp.dot(
            heads_ref[...], piece, preferred_element_type=f32
        )

    theirs = pl.ds(pl.multiple_of((1 - core) * t_dev, t_dev), t_dev)
    mine = pl.ds(pl.multiple_of(core * t_dev, t_dev), t_dev)

    def send_mix():
        mp_send[...] = mix_acc[theirs, :].astype(bf16)
        mp_copy().start()

    def take_mix():
        mp_copy().wait_recv()
        mix_ref[...] = (mix_acc[mine, :] + mp_recv[...].astype(f32)).astype(bf16)

    def finish_units(b):
        size = sizes[b]
        weights = dn[:, :, offsets[b] : offsets[b] + size].reshape(nz * units, size)
        p_send[b, :, :size] = jnp.dot(act[1], weights, preferred_element_type=f32).astype(bf16)
        p_copy(b).start()
        acc[b, :, :size] = jnp.dot(act[0], weights, preferred_element_type=f32)

    def send_home(b):
        p_copy(b).wait_recv()
        size = sizes[b]
        total = acc[b, :, :size] + p_recv[b, :, :size].astype(f32)
        res[b, :, :, :size] = total.astype(bf16).reshape(n_ep, SLOT, size)
        each(1, n_ep, lambda d: res_copy(b, ep, ep_peer(d)).start())
        ret[b, ep, :, :size] = res[b, ep, :, :size]

    c0 = comb_ref[...]
    c_hi = c0.astype(bf16)
    c1 = c0 - c_hi.astype(f32)
    c_mid = c1.astype(bf16)
    c_lo = (c1 - c_mid.astype(f32)).astype(bf16)

    def combine(b):
        each(1, n_ep, lambda d: res_copy(b, ep_peer(d), ep_peer(d)).wait_recv())
        size = sizes[b]
        back = ret[b, :, :, :size].reshape(slots_all, size)
        total = jnp.dot(c_hi, back, preferred_element_type=f32)
        total += jnp.dot(c_mid, back, preferred_element_type=f32)
        total += jnp.dot(c_lo, back, preferred_element_type=f32)
        eo_ref[:, offsets[b] : offsets[b] + size] = total.astype(bf16)

    count = len(down_order)
    issued = 3
    arrived = []
    pending = []
    mixer_work = [gather_heads]
    quarter = -(-n_ep // 4)
    for q in range(4):
        mixer_work.append(
            functools.partial(each, q * quarter, min((q + 1) * quarter, n_ep), project)
        )
    mixer_work += [send_mix, take_mix]
    mixer_at = min(4, count - 8) if count > 8 else 0
    for i in range(count):
        for direction in range(2):
            down_copy(direction, i).wait_recv()
        arrived.append(down_order[i])
        while issued < count:
            b, h = down_order[issued]
            if h > 0 and (b, h - 1) not in arrived:
                break
            start_down(issued)
            issued += 1
        for due, b in [p for p in pending if p[0] <= i]:
            send_home(b)
        pending = [p for p in pending if p[0] > i]
        b, h = down_order[i]
        if h == hops:
            finish_units(b)
            pending.append((i + 2 if i + 4 < count else i + 1, b))
        elif i >= mixer_at and mixer_work:
            mixer_work.pop(0)()
    for due, b in pending:
        send_home(b)
    for work in mixer_work:
        work()

    each(1, nz, lambda d: osl_copy(z, z_peer(d)).wait_send())
    each(1, nz, lambda d: att_copy(z, z_peer(d)).wait_send())
    for direction in range(2):
        for j in range(2):
            gu_first(direction, j).wait_send()
            each(1, hops, lambda h: gu_next(direction, h, j).wait_send())
        gu_last(direction).wait_send()
        for i in range(count):
            down_copy(direction, i).wait_send()
    each(1, n_ep, lambda d: og_copy(ep, ep_peer(d)).wait_send())
    kv_spread.done()
    w_spread.done()
    each(1, n_ep - ep, lambda d: ck_copy(ep, ep + d).wait_send())
    x_copy().wait_send()
    mp_copy().wait_send()
    for b in range(N_BLOCKS):
        p_copy(b).wait_send()
    for b in range(N_BLOCKS):
        combine(b)
    for b in range(N_BLOCKS):
        each(1, n_ep, lambda d: res_copy(b, ep, ep_peer(d)).wait_send())


def local(
    n_ep,
    n_tp,
    queries,
    key_vectors,
    value_vectors,
    cumulative_gate,
    out_weight,
    expert_tokens,
    norm_gain,
    gate_weight,
    up_weight,
    down_weight,
    expert_choice,
    route_weights,
):
    tokens, width = expert_tokens.shape
    block, head = queries.shape
    units = gate_weight.shape[2]
    nz = n_tp // 2
    hops = nz // 2 - 1
    t_dev = block // n_tp
    col = width // n_ep
    part = max(SHARES) * width // 16
    slots_all = n_ep * SLOT
    items = 2 * hops + 1 + len(DOWN_ORDER[hops])
    bf16, f32 = jnp.bfloat16, jnp.float32
    dma = pltpu.SemaphoreType.DMA
    vmem = pltpu.VMEM
    return pl.pallas_call(
        functools.partial(body, n_ep, n_tp),
        out_shape=(
            jax.ShapeDtypeStruct((t_dev, width), bf16),
            jax.ShapeDtypeStruct((tokens, width), bf16),
        ),
        in_specs=[
            pl.BlockSpec(memory_space=vmem if n in (3, 9, 10, 11) else pl.ANY) for n in range(12)
        ],
        out_specs=(pl.BlockSpec(memory_space=vmem),) * 2,
        scratch_shapes=[
            vmem((head, block), bf16),
            vmem((head, block), bf16),
            vmem((head, block), bf16),
            vmem((width, units), bf16),
            vmem((width, units), bf16),
            vmem((head, width), bf16),
            vmem((tokens, width), bf16),
            vmem((block, 128), bf16),
            vmem((block, 1), f32),
            vmem((n_ep, SLOT, width), bf16),
            vmem((tokens, slots_all), f32),
            vmem((n_ep, block, 128), bf16),
            vmem((n_ep, block // 128, 128), f32),
            vmem((2, hops, width, units), bf16),
            vmem((2, hops, width, units), bf16),
            vmem((width, units), bf16),
            vmem((width, units), bf16),
            vmem((nz, units, width), bf16),
            vmem((2, slots_all, nz * units), bf16),
            vmem((2, n_ep, SLOT, width), bf16),
            vmem((N_BLOCKS, slots_all, part), f32),
            vmem((N_BLOCKS, slots_all, part), bf16),
            vmem((N_BLOCKS, slots_all, part), bf16),
            vmem((N_BLOCKS, n_ep, SLOT, part), bf16),
            vmem((N_BLOCKS, n_ep, SLOT, part), bf16),
            vmem((n_ep, nz, head, col), bf16),
            vmem((nz, t_dev, 128), bf16),
            vmem((nz, t_dev, 128), bf16),
            vmem((2 * t_dev, nz * head), bf16),
            vmem((2 * t_dev, width), f32),
            vmem((t_dev, width), bf16),
            vmem((t_dev, width), bf16),
            vmem((block, 128), f32),
            vmem((block, 128), f32),
            vmem((block, 128), f32),
        ]
        + [dma((8,))] * 2
        + [dma((n_ep,))] * 4
        + [dma((8,))] * 2
        + [dma((nz,))] * 4
        + [dma((N_BLOCKS, n_ep))] * 2
        + [dma((2, items))] * 2
        + [dma((2 + N_BLOCKS,))] * 2
        + [dma((8,))],
        compiler_params=pltpu.CompilerParams(
            collective_id=0, has_side_effects=True, vmem_limit_bytes=63 * 2**20
        ),
        name="whole",
    )(
        queries.T,
        key_vectors.T,
        value_vectors.T,
        cumulative_gate.reshape(block // 128, 128),
        gate_weight[0],
        up_weight[0],
        down_weight[0],
        out_weight,
        expert_tokens,
        norm_gain.reshape(1, width),
        expert_choice.T,
        route_weights.T,
    )


def solution(mesh):
    placed = (
        P("ep", "tp"),
        P("ep", "tp"),
        P("ep", "tp"),
        P("ep", "tp"),
        P("tp", None),
        P(("ep", "tp"), None),
        P(),
        P("ep", None, "tp"),
        P("ep", None, "tp"),
        P("ep", "tp", None),
        P(("ep", "tp"), None),
        P(("ep", "tp"), None),
    )
    return jax.shard_map(
        functools.partial(local, mesh.shape["ep"], mesh.shape["tp"]),
        mesh=mesh,
        in_specs=placed,
        out_specs=(P(("ep", "tp"), None), P(("ep", "tp"), None)),
        check_vma=False,
    )
```

```python
import functools
import math

import jax
import jax.numpy as jnp
from jax import lax
from jax.experimental import pallas as pl
from jax.experimental.pallas import tpu as pltpu
from jax.sharding import PartitionSpec as P

SLOT = 16
SIDE = 4
HEAD = 64
MESH = pl.DeviceIdType.MESH

eps_norm = 1e-05
clamp_limit = 7.0
sig_alpha = 1.702
floor_score = -1e30


def gate_row(tile):
    return jnp.concatenate([tile[r : r + 1, :] for r in range(tile.shape[0])], axis=1)


def activate(g, u):
    g = jnp.minimum(g, clamp_limit)
    u = jnp.clip(u, -clamp_limit, clamp_limit)
    return (g * jax.nn.sigmoid(sig_alpha * g) * (u + 1.0)).astype(jnp.bfloat16)


def attend_block(q_ref, cq_ref, kv_ref, ck_ref, m_ref, l_ref, acc_ref, diagonal):
    tile = q_ref.shape[0] // 2
    ck_all_row = gate_row(ck_ref[...])
    for i in range(2):
        rows = pl.ds(i * tile, tile)
        width = (i + 1) * tile if diagonal else kv_ref.shape[0]
        kv = kv_ref[:width, :]
        ck_row = ck_all_row[:, :width]
        s = lax.dot_general(
            q_ref[rows, :], kv, (((1,), (1,)), ((), ())), preferred_element_type=jnp.float32
        )
        s = s + (cq_ref[rows, :] - ck_row)
        if diagonal:
            q_pos = i * tile + lax.broadcasted_iota(jnp.int32, (tile, width), 0)
            k_pos = lax.broadcasted_iota(jnp.int32, (tile, width), 1)
            s = jnp.where(k_pos <= q_pos, s, floor_score)
        top = jnp.max(s, axis=1, keepdims=True)
        if diagonal:
            p = jnp.exp(s - top)
            m_ref[rows, :] = jnp.broadcast_to(top, (tile, 128))
            l_ref[rows, :] = jnp.broadcast_to(jnp.sum(p, axis=1, keepdims=True), (tile, 128))
            acc_ref[rows, :] = jnp.dot(
                p.astype(jnp.bfloat16), kv, preferred_element_type=jnp.float32
            )
        else:
            old = m_ref[rows, :]
            new = jnp.maximum(old, top)
            shrink = jnp.exp(old - new)
            p = jnp.exp(s - new[:, :1])
            m_ref[rows, :] = new
            l_ref[rows, :] = l_ref[rows, :] * shrink + jnp.sum(p, axis=1, keepdims=True)
            acc_ref[rows, :] = acc_ref[rows, :] * shrink + jnp.dot(
                p.astype(jnp.bfloat16), kv, preferred_element_type=jnp.float32
            )


SHARES = (5, 5, 4, 2)
N_BLOCKS = len(SHARES)
DOWN_ORDER = {
    3: ((0, 0), (1, 0), (2, 0), (1, 1), (0, 1), (1, 2), (0, 2), (1, 3), (2, 1), (0, 3),
        (3, 0), (2, 2), (3, 1), (2, 3), (3, 2), (3, 3)),
    1: ((0, 0), (1, 0), (2, 0), (0, 1), (1, 1), (3, 0), (2, 1), (3, 1)),
}


def body(
    n_ep,
    n_tp,
    qt_in,
    kt_in,
    vt_in,
    ck_ref,
    wg_in,
    wu_in,
    wd_in,
    ow_in,
    tok_in,
    gain_ref,
    choice_ref,
    route_ref,
    mix_ref,
    eo_ref,
    qt_ref,
    kt_ref,
    vt_ref,
    wg_ref,
    wu_ref,
    ow_ref,
    tok_ref,
    q_ref,
    cq_ref,
    og_ref,
    comb_ref,
    kv_all,
    ck_all,
    rg,
    ru,
    lg,
    lu,
    dn,
    act,
    x,
    acc,
    p_send,
    p_recv,
    res,
    ret,
    w_all,
    att_send,
    att_in,
    heads_ref,
    mix_acc,
    mp_send,
    mp_recv,
    m_ref,
    l_ref,
    att_acc,
    s_kv,
    r_kv,
    s_ck,
    r_ck,
    s_og,
    r_og,
    s_w,
    r_w,
    s_osl,
    r_osl,
    s_att,
    r_att,
    s_res,
    r_res,
    s_ring,
    r_ring,
    s_pt,
    r_pt,
    s_in,
):
    bf16, f32 = jnp.bfloat16, jnp.float32
    nz = n_tp // 2
    hops = nz // 2 - 1
    ep = lax.axis_index("ep")
    tp = lax.axis_index("tp")
    z = lax.div(tp, 2)
    core = lax.rem(tp, 2)
    right = lax.rem(tp + 2, n_tp)
    left = lax.rem(tp + n_tp - 2, n_tp)
    partner = tp + 1 - 2 * core
    units, width = wd_in.shape
    block = q_ref.shape[0]
    tokens = tok_ref.shape[0]
    slots_all = n_ep * SLOT
    col = width // n_ep
    unit = width // 16
    sizes = [n * unit for n in SHARES]
    offsets = [sum(sizes[:b]) for b in range(N_BLOCKS)]
    t_dev = mp_send.shape[0]

    def ep_peer(d):
        return lax.rem(ep + d, n_ep)

    def z_peer(d):
        return lax.rem(z + d, nz)

    def ep_copy(src, dst, send, recv, peer):
        return pltpu.make_async_remote_copy(
            src_ref=src, dst_ref=dst, send_sem=send, recv_sem=recv,
            device_id={"ep": peer}, device_id_type=MESH,
        )

    def tp_copy(src, dst, send, recv, peer):
        return pltpu.make_async_remote_copy(
            src_ref=src, dst_ref=dst, send_sem=send, recv_sem=recv,
            device_id={"tp": peer}, device_id_type=MESH,
        )

    y = lax.div(ep, SIDE)
    x_at = lax.rem(ep, SIDE)
    x_next = y * SIDE + lax.rem(x_at + 1, SIDE)
    x_prev = y * SIDE + lax.rem(x_at + SIDE - 1, SIDE)
    x_far = y * SIDE + lax.rem(x_at + 2, SIDE)
    y_next = lax.rem(y + 1, SIDE)
    y_prev = lax.rem(y + SIDE - 1, SIDE)
    y_far = lax.rem(y + 2, SIDE)

    class Spread:
        def __init__(self, buf, send, recv):
            self.buf, self.send, self.recv = buf, send, recv
            self.half = buf.shape[1] // 2

        def move(self, n, region, peer):
            return ep_copy(region, region, self.send.at[n], self.recv.at[n], peer)

        def part(self, slot, n):
            return self.buf.at[slot, pl.ds(n * self.half, self.half)]

        def rows(self, row, n, count):
            return self.buf.at[pl.ds(row * SIDE + n, count)]

        def sent(self, step):
            if step == 1:
                return (
                    self.move(0, self.buf.at[ep], x_next),
                    self.move(1, self.buf.at[ep], x_prev),
                )
            if step == 2:
                return (
                    self.move(2, self.part(x_prev, 0), x_next),
                    self.move(3, self.part(x_next, 1), x_prev),
                )
            up, down = y_next * SIDE + x_at, y_prev * SIDE + x_at
            if step == 3:
                return (
                    self.move(4, self.rows(y, 0, SIDE), up),
                    self.move(5, self.rows(y, 0, SIDE), down),
                )
            return (
                self.move(6, self.rows(y_prev, 0, SIDE // 2), up),
                self.move(7, self.rows(y_next, SIDE // 2, SIDE // 2), down),
            )

        def come(self, step):
            if step == 1:
                return (
                    self.move(0, self.buf.at[x_prev], x_next),
                    self.move(1, self.buf.at[x_next], x_prev),
                )
            if step == 2:
                return (
                    self.move(2, self.part(x_far, 0), x_next),
                    self.move(3, self.part(x_far, 1), x_prev),
                )
            up, down = y_next * SIDE + x_at, y_prev * SIDE + x_at
            if step == 3:
                return (
                    self.move(4, self.rows(y_prev, 0, SIDE), up),
                    self.move(5, self.rows(y_next, 0, SIDE), down),
                )
            return (
                self.move(6, self.rows(y_far, 0, SIDE // 2), up),
                self.move(7, self.rows(y_far, SIDE // 2, SIDE // 2), down),
            )

        def wait(self, step):
            for copy in self.come(step):
                copy.wait_recv()

        def start(self, step):
            for copy in self.sent(step):
                copy.start()

        def done(self):
            for step in range(1, 5):
                for copy in self.sent(step):
                    copy.wait_send()

    kv_spread = Spread(kv_all, s_kv, r_kv)
    w_spread = Spread(w_all, s_w, r_w)

    def ck_copy(slot, peer):
        return ep_copy(ck_ref, ck_all.at[slot], s_ck.at[peer], r_ck.at[slot], peer)

    def og_copy(slot, peer):
        return ep_copy(og_ref.at[peer], x.at[0, slot], s_og.at[peer], r_og.at[slot], peer)

    def res_copy(b, slot, peer):
        return ep_copy(
            res.at[b, peer, :, pl.ds(0, sizes[b])],
            ret.at[b, slot, :, pl.ds(0, sizes[b])],
            s_res.at[b, peer], r_res.at[b, slot], peer
        )

    my_cols = pl.ds(pl.multiple_of(ep * col, col), col)

    def osl_copy(slot, pz):
        return tp_copy(
            ow_ref.at[:, my_cols], w_all.at[ep, slot], s_osl.at[pz], r_osl.at[slot], 2 * pz + core
        )

    def att_copy(slot, pz):
        return tp_copy(
            att_send.at[pz], att_in.at[slot], s_att.at[pz], r_att.at[slot], 2 * pz + core
        )

    def pt_copy(src, dst, n):
        return tp_copy(src, dst, s_pt.at[n], r_pt.at[n], partner)

    def x_copy():
        return pt_copy(x.at[0], x.at[1], 0)

    def mp_copy():
        return pt_copy(mp_send, mp_recv, 1)

    def p_copy(b):
        cols = pl.ds(0, sizes[b])
        return pt_copy(p_send.at[b, :, cols], p_recv.at[b, :, cols], 2 + b)

    peers = (right, left)
    own = (wg_ref, wu_ref)
    slots = (rg, ru)
    last = (lg, lu)
    firsts = 2 * hops + 1
    down_order = DOWN_ORDER[hops]
    items = firsts + len(down_order)

    def gu_copy(direction, h, j):
        a = j if direction == 0 else 1 - j
        n = 2 * h + j
        sems = (s_ring.at[direction, n], r_ring.at[direction, n])
        return lambda src, dst: tp_copy(src, dst, *sems, peers[direction]), a

    def gu_first(direction, j):
        make, a = gu_copy(direction, 0, j)
        return make(own[a], slots[a].at[direction, 0])

    def gu_next(direction, h, j):
        make, a = gu_copy(direction, h, j)
        return make(slots[a].at[direction, h - 1], slots[a].at[direction, h])

    def gu_last(direction):
        make, a = gu_copy(direction, hops, 0)
        return make(slots[a].at[direction, hops - 1], last[a])

    def down_copy(direction, i):
        b, h = down_order[i]
        cols = pl.ds(offsets[b], sizes[b])
        n = firsts + i
        rows = pl.ds(0, units)
        to = 1 + 2 * h + direction
        if h == hops:
            rows = pl.ds(direction * (units // 2), units // 2)
            to = 1 + 2 * hops
        if h == 0:
            src = dn.at[0, rows, cols]
        else:
            src = dn.at[1 + 2 * (h - 1) + direction, rows, cols]
        return tp_copy(
            src, dn.at[to, rows, cols], s_ring.at[direction, n], r_ring.at[direction, n],
            peers[direction],
        )

    def start_down(i):
        for direction in range(2):
            down_copy(direction, i).start()

    def each(start, stop, fn):
        def run(d, carry):
            fn(d)
            return carry

        lax.fori_loop(start, stop, run, 0)

    loads = [
        pltpu.make_async_copy(src, dst, s_in.at[n])
        for n, (src, dst) in enumerate(
            (
                (wg_in, wg_ref),
                (wu_in, wu_ref),
                (ow_in, ow_ref),
                (kt_in, kt_ref),
                (vt_in, vt_ref),
                (qt_in, qt_ref),
                (tok_in, tok_ref),
                (wd_in, dn.at[0]),
            )
        )
    ]
    for load in loads:
        load.start()

    barrier = pltpu.get_barrier_semaphore()
    each(
        1, n_ep,
        lambda d: pl.semaphore_signal(
            barrier, inc=1, device_id={"ep": ep_peer(d)}, device_id_type=MESH
        ),
    )
    each(
        1, nz,
        lambda d: pl.semaphore_signal(
            barrier, inc=1, device_id={"tp": 2 * z_peer(d) + core}, device_id_type=MESH
        ),
    )
    pl.semaphore_signal(barrier, inc=1, device_id={"tp": partner}, device_id_type=MESH)
    pl.semaphore_wait(barrier, n_ep - 1 + nz - 1 + 1)

    for load in loads[:3]:
        load.wait()
    for direction in range(2):
        gu_first(direction, 0).start()
    each(1, nz, lambda d: osl_copy(z, z_peer(d)).start())
    for direction in range(2):
        gu_first(direction, 1).start()
    for load in loads[3:]:
        load.wait()

    kv_all[ep] = (
        jnp.concatenate([kt_ref[...].astype(f32), vt_ref[...].astype(f32)], axis=0)
        .T.astype(bf16)
    )
    scaled = qt_ref[...].astype(f32) * (1.0 / math.sqrt(HEAD))
    q_ref[...] = jnp.concatenate([scaled, jnp.zeros_like(scaled)], axis=0).T.astype(bf16)
    turned = ck_ref[...].T
    for r in range(block // 128):
        cq_ref[pl.ds(r * 128, 128), :] = turned[:, r : r + 1]

    ids = choice_ref[...]
    e_pos = lax.broadcasted_iota(jnp.int32, (n_ep, tokens), 0)
    named = [(e_pos == ids[k : k + 1, :]).astype(f32) for k in range(ids.shape[0])]
    both = functools.reduce(jnp.add, named)
    before = (
        lax.broadcasted_iota(jnp.int32, (tokens, tokens), 0)
        < lax.broadcasted_iota(jnp.int32, (tokens, tokens), 1)
    )
    earlier = jnp.dot(
        both.astype(bf16), before.astype(f32).astype(bf16), preferred_element_type=f32
    )
    s_pos = lax.broadcasted_iota(jnp.int32, (slots_all, tokens), 0).astype(f32)
    placing = jnp.zeros((slots_all, tokens), f32)
    comb = jnp.zeros((slots_all, tokens), f32)
    for k in range(ids.shape[0]):
        rank = jnp.sum(named[k] * earlier, axis=0, keepdims=True)
        slot = ids[k : k + 1, :].astype(f32) * SLOT + rank
        here = s_pos == slot
        placing = jnp.where(here, 1.0, placing)
        comb = jnp.where(here, route_ref[k : k + 1, :], comb)
    comb_ref[...] = comb.T
    tok = tok_ref[...].astype(f32)
    normed = (
        tok * lax.rsqrt(jnp.mean(tok * tok, axis=1, keepdims=True) + eps_norm) * gain_ref[...]
    ).astype(bf16)
    og_ref[...] = (
        jnp.dot(placing.astype(bf16), normed, preferred_element_type=f32)
        .astype(bf16)
        .reshape(n_ep, SLOT, width)
    )

    attend_block(q_ref, cq_ref, kv_all.at[ep], ck_ref, m_ref, l_ref, att_acc, True)

    kv_spread.start(1)
    each(1, n_ep - ep, lambda d: ck_copy(ep, ep + d).start())
    each(1, n_ep, lambda d: og_copy(ep, ep_peer(d)).start())
    x[0, ep] = og_ref[ep]
    w_all[ep, z] = ow_ref[:, my_cols]

    def attend_step(j):
        ck_copy(j, j).wait_recv()
        attend_block(q_ref, cq_ref, kv_all.at[j], ck_all.at[j], m_ref, l_ref, att_acc, False)

    def expert_units(g_ref, u_ref, n):
        cols = pl.ds(pl.multiple_of(n * units, units), units)
        for half in range(2):
            rows = x[half].reshape(slots_all, width)
            g = jnp.dot(rows, g_ref[...], preferred_element_type=f32)
            u = jnp.dot(rows, u_ref[...], preferred_element_type=f32)
            act[half, :, cols] = activate(g, u)

    def units_of(h):
        for direction in range(2):
            expert_units(rg.at[direction, h], ru.at[direction, h], 1 + 2 * h + direction)

    def kv_step(step):
        kv_spread.wait(step - 1)
        kv_spread.start(step)

    def w_step(step):
        w_spread.wait(step - 1)
        w_spread.start(step)

    def first_w():
        each(1, nz, lambda d: osl_copy(z_peer(d), z_peer(d)).wait_recv())
        w_spread.start(1)

    def swap_rows():
        each(1, n_ep, lambda d: og_copy(ep_peer(d), ep_peer(d)).wait_recv())
        x_copy().start()

    def own_units():
        x_copy().wait_recv()
        expert_units(wg_ref, wu_ref, 0)

    def send_attention():
        for pz in range(nz):
            rows = pl.ds(pz * 2 * t_dev, 2 * t_dev)
            o = (att_acc[rows, :] / l_ref[rows, :])[:, HEAD:]
            att_send[pz] = jnp.concatenate([o[:t_dev], o[t_dev:]], axis=1).astype(bf16)
        att_in[z] = att_send[z]

    def above(n):
        return SIDE * jnp.maximum(y - n, 0)

    def units_safe(h):
        if h < hops:
            units_of(h)

    work_list = [
        (0, lambda: kv_step(2)),
        (0, first_w),
        (1, lambda: kv_step(3)),
        (1, swap_rows),
        (1, lambda: each(SIDE * y, ep, attend_step)),
        (1, lambda: w_step(2)),
        (2, own_units),
        (2, lambda: units_safe(0)),
        (3, lambda: kv_step(4)),
        (3, lambda: each(above(1), SIDE * y, attend_step)),
        (4, lambda: w_step(3)),
        (4, lambda: units_safe(1)),
        (4, lambda: each(0, above(2), attend_step)),
        (5, lambda: kv_spread.wait(4)),
        (5, lambda: each(above(2), above(1), attend_step)),
        (6, send_attention),
        (6, lambda: w_step(4)),
        (6, lambda: units_safe(2)),
    ]
    for n in range(firsts):
        h, j = n // 2, n % 2
        for direction in range(2):
            if n == firsts - 1:
                gu_last(direction).wait_recv()
            elif h == 0:
                gu_first(direction, j).wait_recv()
            else:
                gu_next(direction, h, j).wait_recv()
            follow = n + 2
            if follow < firsts - 1:
                gu_next(direction, h + 1, j).start()
            elif follow == firsts - 1:
                gu_last(direction).start()
        if n == firsts - 2:
            for i in range(3):
                start_down(i)
        for at, work in work_list:
            if min(at, firsts - 1) == n:
                work()
    expert_units(lg, lu, 1 + 2 * hops)

    def gather_heads():
        each(1, nz, lambda d: att_copy(z_peer(d), z_peer(d)).wait_recv())
        got = [att_in[pz].astype(f32) for pz in range(nz)]
        heads_ref[pl.ds(0, t_dev), :] = jnp.concatenate(
            [t[:, :HEAD] for t in got], axis=1
        ).astype(bf16)
        heads_ref[pl.ds(t_dev, t_dev), :] = jnp.concatenate(
            [t[:, HEAD:] for t in got], axis=1
        ).astype(bf16)
        w_spread.wait(4)

    def project(e):
        piece = w_all[e].reshape(nz * HEAD, col)
        mix_acc[:, pl.ds(pl.multiple_of(e * col, col), col)] = jnp.dot(
            heads_ref[...], piece, preferred_element_type=f32
        )

    theirs = pl.ds(pl.multiple_of((1 - core) * t_dev, t_dev), t_dev)
    mine = pl.ds(pl.multiple_of(core * t_dev, t_dev), t_dev)

    def send_mix():
        mp_send[...] = mix_acc[theirs, :].astype(bf16)
        mp_copy().start()

    def take_mix():
        mp_copy().wait_recv()
        mix_ref[...] = (mix_acc[mine, :] + mp_recv[...].astype(f32)).astype(bf16)

    def finish_units(b):
        size = sizes[b]
        weights = dn[:, :, offsets[b] : offsets[b] + size].reshape(nz * units, size)
        p_send[b, :, :size] = jnp.dot(act[1], weights, preferred_element_type=f32).astype(bf16)
        p_copy(b).start()
        acc[b, :, :size] = jnp.dot(act[0], weights, preferred_element_type=f32)

    def send_home(b):
        p_copy(b).wait_recv()
        size = sizes[b]
        total = acc[b, :, :size] + p_recv[b, :, :size].astype(f32)
        res[b, :, :, :size] = total.astype(bf16).reshape(n_ep, SLOT, size)
        each(1, n_ep, lambda d: res_copy(b, ep, ep_peer(d)).start())
        ret[b, ep, :, :size] = res[b, ep, :, :size]

    c0 = comb_ref[...]
    c_hi = c0.astype(bf16)
    c1 = c0 - c_hi.astype(f32)
    c_mid = c1.astype(bf16)
    c_lo = (c1 - c_mid.astype(f32)).astype(bf16)

    def combine(b):
        each(1, n_ep, lambda d: res_copy(b, ep_peer(d), ep_peer(d)).wait_recv())
        size = sizes[b]
        back = ret[b, :, :, :size].reshape(slots_all, size)
        total = jnp.dot(c_hi, back, preferred_element_type=f32)
        total += jnp.dot(c_mid, back, preferred_element_type=f32)
        total += jnp.dot(c_lo, back, preferred_element_type=f32)
        eo_ref[:, offsets[b] : offsets[b] + size] = total.astype(bf16)

    count = len(down_order)
    issued = 3
    arrived = []
    pending = []
    mixer_work = [gather_heads]
    quarter = -(-n_ep // 4)
    for q in range(4):
        mixer_work.append(
            functools.partial(each, q * quarter, min((q + 1) * quarter, n_ep), project)
        )
    mixer_work += [send_mix, take_mix]
    mixer_at = count
    for i in range(count):
        for direction in range(2):
            down_copy(direction, i).wait_recv()
        arrived.append(down_order[i])
        while issued < count:
            b, h = down_order[issued]
            if h > 0 and (b, h - 1) not in arrived:
                break
            start_down(issued)
            issued += 1
        if i == count - 4:
            each(1, nz, lambda d: att_copy(z, z_peer(d)).start())
        for due, b in [p for p in pending if p[0] <= i]:
            send_home(b)
        pending = [p for p in pending if p[0] > i]
        b, h = down_order[i]
        if h == hops:
            finish_units(b)
            pending.append((i + 2 if i + 4 < count else i + 1, b))
        elif i >= mixer_at and mixer_work:
            mixer_work.pop(0)()
    for due, b in pending:
        send_home(b)
    for work in mixer_work[:-1]:
        work()

    each(1, nz, lambda d: osl_copy(z, z_peer(d)).wait_send())
    each(1, nz, lambda d: att_copy(z, z_peer(d)).wait_send())
    for direction in range(2):
        for j in range(2):
            gu_first(direction, j).wait_send()
            each(1, hops, lambda h: gu_next(direction, h, j).wait_send())
        gu_last(direction).wait_send()
        for i in range(count):
            down_copy(direction, i).wait_send()
    each(1, n_ep, lambda d: og_copy(ep, ep_peer(d)).wait_send())
    kv_spread.done()
    w_spread.done()
    each(1, n_ep - ep, lambda d: ck_copy(ep, ep + d).wait_send())
    x_copy().wait_send()
    for b in range(N_BLOCKS):
        p_copy(b).wait_send()
    for b in range(N_BLOCKS - 1):
        combine(b)
    take_mix()
    combine(N_BLOCKS - 1)
    mp_copy().wait_send()
    for b in range(N_BLOCKS):
        each(1, n_ep, lambda d: res_copy(b, ep, ep_peer(d)).wait_send())


def local(
    n_ep,
    n_tp,
    queries,
    key_vectors,
    value_vectors,
    cumulative_gate,
    out_weight,
    expert_tokens,
    norm_gain,
    gate_weight,
    up_weight,
    down_weight,
    expert_choice,
    route_weights,
):
    tokens, width = expert_tokens.shape
    block, head = queries.shape
    units = gate_weight.shape[2]
    nz = n_tp // 2
    hops = nz // 2 - 1
    t_dev = block // n_tp
    col = width // n_ep
    part = max(SHARES) * width // 16
    slots_all = n_ep * SLOT
    items = 2 * hops + 1 + len(DOWN_ORDER[hops])
    bf16, f32 = jnp.bfloat16, jnp.float32
    dma = pltpu.SemaphoreType.DMA
    vmem = pltpu.VMEM
    return pl.pallas_call(
        functools.partial(body, n_ep, n_tp),
        out_shape=(
            jax.ShapeDtypeStruct((t_dev, width), bf16),
            jax.ShapeDtypeStruct((tokens, width), bf16),
        ),
        in_specs=[
            pl.BlockSpec(memory_space=vmem if n in (3, 9, 10, 11) else pl.ANY) for n in range(12)
        ],
        out_specs=(pl.BlockSpec(memory_space=vmem),) * 2,
        scratch_shapes=[
            vmem((head, block), bf16),
            vmem((head, block), bf16),
            vmem((head, block), bf16),
            vmem((width, units), bf16),
            vmem((width, units), bf16),
            vmem((head, width), bf16),
            vmem((tokens, width), bf16),
            vmem((block, 128), bf16),
            vmem((block, 1), f32),
            vmem((n_ep, SLOT, width), bf16),
            vmem((tokens, slots_all), f32),
            vmem((n_ep, block, 128), bf16),
            vmem((n_ep, block // 128, 128), f32),
            vmem((2, hops, width, units), bf16),
            vmem((2, hops, width, units), bf16),
            vmem((width, units), bf16),
            vmem((width, units), bf16),
            vmem((nz, units, width), bf16),
            vmem((2, slots_all, nz * units), bf16),
            vmem((2, n_ep, SLOT, width), bf16),
            vmem((N_BLOCKS, slots_all, part), f32),
            vmem((N_BLOCKS, slots_all, part), bf16),
            vmem((N_BLOCKS, slots_all, part), bf16),
            vmem((N_BLOCKS, n_ep, SLOT, part), bf16),
            vmem((N_BLOCKS, n_ep, SLOT, part), bf16),
            vmem((n_ep, nz, head, col), bf16),
            vmem((nz, t_dev, 128), bf16),
            vmem((nz, t_dev, 128), bf16),
            vmem((2 * t_dev, nz * head), bf16),
            vmem((2 * t_dev, width), f32),
            vmem((t_dev, width), bf16),
            vmem((t_dev, width), bf16),
            vmem((block, 128), f32),
            vmem((block, 128), f32),
            vmem((block, 128), f32),
        ]
        + [dma((8,))] * 2
        + [dma((n_ep,))] * 4
        + [dma((8,))] * 2
        + [dma((nz,))] * 4
        + [dma((N_BLOCKS, n_ep))] * 2
        + [dma((2, items))] * 2
        + [dma((2 + N_BLOCKS,))] * 2
        + [dma((8,))],
        compiler_params=pltpu.CompilerParams(
            collective_id=0, has_side_effects=True, vmem_limit_bytes=63 * 2**20
        ),
        name="whole",
    )(
        queries.T,
        key_vectors.T,
        value_vectors.T,
        cumulative_gate.reshape(block // 128, 128),
        gate_weight[0],
        up_weight[0],
        down_weight[0],
        out_weight,
        expert_tokens,
        norm_gain.reshape(1, width),
        expert_choice.T,
        route_weights.T,
    )


def solution(mesh):
    placed = (
        P("ep", "tp"),
        P("ep", "tp"),
        P("ep", "tp"),
        P("ep", "tp"),
        P("tp", None),
        P(("ep", "tp"), None),
        P(),
        P("ep", None, "tp"),
        P("ep", None, "tp"),
        P("ep", "tp", None),
        P(("ep", "tp"), None),
        P(("ep", "tp"), None),
    )
    return jax.shard_map(
        functools.partial(local, mesh.shape["ep"], mesh.shape["tp"]),
        mesh=mesh,
        in_specs=placed,
        out_specs=(P(("ep", "tp"), None), P(("ep", "tp"), None)),
        check_vma=False,
    )
```
